32 devices in a mesh: rep: 2 (over x), fs: 8 (over z, y), tp: 2 (over core).
Axes of the slice: x: 2, y: 2, z: 4, core: 2. Of those that a mesh axis runs over, the one named last changes fastest.
Arguments:
- incoming_features: bfloat16 [3072, 2048], P(('rep', 'fs'), 'tp'), may hold values from -6 to 6
- attend_prenormal_scale: bfloat16 [2048], replicated, may hold values from 0.099609375 to 1.8984375
- probe_matrix: bfloat16 [2048, 512], P('fs', 'tp'), may hold values from -0.125 to 0.125
- lookup_matrix: bfloat16 [2048, 512], P('fs', 'tp'), may hold values from -0.125 to 0.125
- content_matrix: bfloat16 [2048, 1024], P('fs', 'tp'), may hold values from -0.125 to 0.125
- forgetting_matrix: bfloat16 [2048, 512], P('fs', 'tp'), may hold values from -0.125 to 0.125
- result_switch_matrix: bfloat16 [2048, 1024], P('fs', 'tp'), may hold values from -0.125 to 0.125
- forgetting_shift: float32 [512], P('tp'), may hold values from -0.5 to 5.5
- spike_forget_logarithm: float32 [3072, 512], P(('rep', 'fs'), 'tp'), may hold values from -0.7 to 0
- attend_unit_scale: bfloat16 [1024], P('tp'), may hold values from 0.099609375 to 1.8984375
- attend_result_matrix: bfloat16 [1024, 2048], P('tp', 'fs'), may hold values from -0.1875 to 0.1875
- perceptron_scale: bfloat16 [2048], replicated, may hold values from 0.099609375 to 1.8984375
- content_expand_matrix: bfloat16 [2048, 4096], P('fs', 'tp'), may hold values from -0.125 to 0.125
- switch_expand_matrix: bfloat16 [2048, 4096], P('fs', 'tp'), may hold values from -0.125 to 0.125
- content_kernel: bfloat16 [3, 4096], P(None, 'tp'), may hold values from -3.5 to 3.5
- switch_kernel: bfloat16 [3, 4096], P(None, 'tp'), may hold values from -3.5 to 3.5
- contract_matrix: bfloat16 [4096, 2048], P('tp', 'fs'), may hold values from -0.09375 to 0.09375
Outputs:
- out_rows: bfloat16 [3072, 2048], P(('rep', 'fs'), 'tp')
The draws below stay inside these ranges and needn't reach their ends.
All inputs are finite; a program needn't handle non-finite values.
Results may differ from the reference program's by a relative error of at most 0.02.
Values may be sent and summed in bfloat16 or wider, within the bound.
No kernel may reach another device: no remote copies, remote signals or barrier semaphores. Data moves between devices by JAX's collectives and lax.ppermute only.
A program may use at most 64 MiB of HBM per device.

```python
import math
import jax
import jax.numpy as jnp
from jax import lax

EMBED_DIM = 2048
HEAD_K = 32
HEAD_V = 64
FF = 4096
BLOCK = 64
CONTEXT_SPAN = 192
LOOKUP_FEATURES = 512
VAL_W = 1024
BATCH_SIZE = 16
TOKENS = 3072
N_TP = 2


def draw_forgetting_shift(key, part):
    head_count = LOOKUP_FEATURES // HEAD_K
    key_slow, key_high, key_low = jax.random.split(jax.random.fold_in(key, 11), 3)
    slow = jax.random.uniform(key_slow, (head_count,)) < 0.5
    slow_channels = jnp.repeat(slow, HEAD_K)
    high = jax.random.uniform(key_high, (LOOKUP_FEATURES,), jnp.float32, 3.5, 5.5)
    low = jax.random.uniform(key_low, (LOOKUP_FEATURES,), jnp.float32, -0.5, 1.0)
    return jnp.where(slow_channels, high, low).astype(jnp.float32)


def draw_spike_forget_logarithm(key, part):
    head_count = LOOKUP_FEATURES // HEAD_K
    key_hit, key_depth = jax.random.split(jax.random.fold_in(key, 23))
    hits = jax.random.uniform(key_hit, (TOKENS, head_count)) < 6.0 / CONTEXT_SPAN
    depth = jax.random.uniform(key_depth, (TOKENS, head_count), jnp.float32, math.log(0.5), math.log(0.8))
    return jnp.repeat(jnp.where(hits, depth, 0.0), HEAD_K, axis=1).astype(jnp.float32)


def level_of(own_key, shape, pieces, smallest, top_value):
    factor_of, own = 1.0, jax.random.fold_in(own_key, 6)
    for position, parts in pieces:
        steps = jnp.exp(jax.random.uniform(jax.random.fold_in(own, position), (parts,), jnp.float32, smallest / len(pieces), top_value / len(pieces)))
        factor_of = factor_of * jnp.repeat(steps, shape[position] // parts).reshape([-1 if axis == position else 1 for axis in range(len(shape))])
    return factor_of


def gaussian(own_key, dims, spread, limit, cuts=(), held_as=jnp.bfloat16):
    factor_of = level_of(own_key, dims, cuts, -0.22, 0.18) if cuts else 1.0
    values = jax.random.normal(own_key, dims, jnp.float32) * spread * factor_of
    return jnp.minimum(jnp.maximum(values, -limit), limit).astype(held_as)


def setup_inputs(seed: int = 0) -> dict:
    streams_of = jax.random.split(jax.random.key(seed), 18)
    incoming_features = gaussian(streams_of[0], (TOKENS, EMBED_DIM), 1.0, 6.0, ((0, 16), (1, 2)))
    attend_prenormal_scale = jnp.clip(1.0 + 0.18 * jax.random.normal(streams_of[1], (EMBED_DIM,), jnp.float32), 0.099609375, 1.8984375).astype(jnp.bfloat16)
    probe_matrix = gaussian(streams_of[2], (EMBED_DIM, LOOKUP_FEATURES), EMBED_DIM ** -0.5, 0.125, ((0, 8), (1, 2)))
    lookup_matrix = gaussian(streams_of[3], (EMBED_DIM, LOOKUP_FEATURES), EMBED_DIM ** -0.5, 0.125, ((0, 8), (1, 2)))
    content_matrix = gaussian(streams_of[4], (EMBED_DIM, VAL_W), EMBED_DIM ** -0.5, 0.125, ((0, 8), (1, 2)))
    forgetting_matrix = gaussian(streams_of[5], (EMBED_DIM, LOOKUP_FEATURES), EMBED_DIM ** -0.5, 0.125, ((0, 8), (1, 2)))
    result_switch_matrix = gaussian(streams_of[6], (EMBED_DIM, VAL_W), EMBED_DIM ** -0.5, 0.125, ((0, 8), (1, 2)))
    forgetting_shift = draw_forgetting_shift(jax.random.fold_in(streams_of[17], 71), 0)
    spike_forget_logarithm = draw_spike_forget_logarithm(jax.random.fold_in(streams_of[17], 71), 0)
    attend_unit_scale = jnp.clip(1.0 + 0.18 * jax.random.normal(streams_of[9], (VAL_W,), jnp.float32), 0.099609375, 1.8984375).astype(jnp.bfloat16)
    attend_result_matrix = gaussian(streams_of[10], (VAL_W, EMBED_DIM), VAL_W ** -0.5, 0.1875, ((0, 2), (1, 8)))
    perceptron_scale = jnp.clip(1.0 + 0.18 * jax.random.normal(streams_of[11], (EMBED_DIM,), jnp.float32), 0.099609375, 1.8984375).astype(jnp.bfloat16)
    content_expand_matrix = gaussian(streams_of[12], (EMBED_DIM, FF), EMBED_DIM ** -0.5, 0.125, ((0, 8), (1, 2)))
    switch_expand_matrix = gaussian(streams_of[13], (EMBED_DIM, FF), EMBED_DIM ** -0.5, 0.125, ((0, 8), (1, 2)))
    content_kernel = gaussian(streams_of[14], (3, FF), 3 ** -0.5, 3.5, ((1, 2),))
    switch_kernel = gaussian(streams_of[15], (3, FF), 3 ** -0.5, 3.5, ((1, 2),))
    contract_matrix = gaussian(streams_of[16], (FF, EMBED_DIM), FF ** -0.5, 0.09375, ((0, 2), (1, 8)))
    return {"incoming_features": incoming_features, "attend_prenormal_scale": attend_prenormal_scale, "probe_matrix": probe_matrix, "lookup_matrix": lookup_matrix, "content_matrix": content_matrix, "forgetting_matrix": forgetting_matrix, "result_switch_matrix": result_switch_matrix, "forgetting_shift": forgetting_shift, "spike_forget_logarithm": spike_forget_logarithm, "attend_unit_scale": attend_unit_scale, "attend_result_matrix": attend_result_matrix, "perceptron_scale": perceptron_scale, "content_expand_matrix": content_expand_matrix, "switch_expand_matrix": switch_expand_matrix, "content_kernel": content_kernel, "switch_kernel": switch_kernel, "contract_matrix": contract_matrix}


norm_eps = 1e-06
switch_multiplier = 16.0

def row_norm(content_tokens, gain):
    content_tokens = content_tokens.astype(jnp.float32)
    scaled = content_tokens * lax.rsqrt(lax.optimization_barrier(jnp.mean(content_tokens * content_tokens, axis=-1, keepdims=True)) + norm_eps)
    return (scaled * gain.astype(jnp.float32)).astype(jnp.bfloat16)

def gated_scan(probe_tokens, lookup_tokens, content_tokens, forgetting_scores):
    length, heads, key_size = probe_tokens.shape
    value_size = content_tokens.shape[-1]
    blocks = length // BLOCK

    def split_blocks(array):
        return array.reshape(blocks, BLOCK, heads, array.shape[-1])
    causal = jnp.arange(BLOCK)[:, None] >= jnp.arange(BLOCK)[None, :]
    highest = lax.Precision.HIGHEST

    def step(state, incoming_tokens):
        query_block, key_block, value_block, decay_block = incoming_tokens
        cumulative = jnp.cumsum(decay_block, axis=0)
        differ = cumulative[:, None] - cumulative[None, :]
        weight = jnp.exp(jnp.where(causal[:, :, None, None], differ, -jnp.inf))
        scores = jnp.einsum('thd,shd,tshd->tsh', query_block, key_block, weight, precision=highest)
        inner = jnp.einsum('tsh,shv->thv', scores, value_block, precision=highest)
        carried = jnp.einsum('thd,hdv->thv', query_block * jnp.exp(cumulative), state, precision=highest)
        final = cumulative[-1]
        state = jnp.exp(final)[:, :, None] * state + jnp.einsum('shd,shv->hdv', key_block * jnp.exp(final[None] - cumulative), value_block, precision=highest)
        return (state, inner + carried)
    start_state = jnp.zeros((heads, key_size, value_size), jnp.float32)
    _, result_tokens = lax.scan(step, start_state, (split_blocks(probe_tokens), split_blocks(lookup_tokens), split_blocks(content_tokens), split_blocks(forgetting_scores)))
    return result_tokens.reshape(length, heads, value_size)

def attend_unit_results(probe_tokens, lookup_tokens, content_tokens, result_switch, forgetting_raw, spike_forgetting, attend_unit_scale):
    length = probe_tokens.shape[0]
    heads = probe_tokens.shape[1] // HEAD_K
    forgetting_scores = jax.nn.log_sigmoid(forgetting_raw) / switch_multiplier + spike_forgetting

    def split_heads(array, width):
        return array.astype(jnp.float32).reshape(length, heads, width)
    result_tokens = gated_scan(split_heads(probe_tokens, HEAD_K) * HEAD_K ** (-0.5), split_heads(lookup_tokens, HEAD_K), split_heads(content_tokens, HEAD_V), split_heads(forgetting_scores, HEAD_K))
    result_tokens = result_tokens * lax.rsqrt(lax.optimization_barrier(jnp.mean(result_tokens * result_tokens, axis=-1, keepdims=True)) + norm_eps)
    result_tokens = result_tokens * attend_unit_scale.astype(jnp.float32).reshape(heads, HEAD_V)
    switched_result = result_tokens.reshape(length, heads * HEAD_V) * jax.nn.silu(result_switch.astype(jnp.float32))
    return switched_result.astype(jnp.bfloat16)

def causal_conv(content_tokens, taps):
    content_tokens = content_tokens.astype(jnp.float32)
    taps = taps.astype(jnp.float32)
    width = taps.shape[0]
    padded = jnp.pad(content_tokens, ((width - 1, 0), (0, 0)))
    total = jnp.zeros_like(content_tokens)
    for offset in range(width):
        total = total + padded[offset:offset + content_tokens.shape[0]] * taps[offset]
    return total

def grouped_product(content_tokens, weight):
    group = content_tokens.shape[1] // N_TP
    total = jnp.zeros((content_tokens.shape[0], weight.shape[1]), jnp.float32)
    for index in range(N_TP):
        partial_sum = jnp.dot(content_tokens[:, index * group:(index + 1) * group], weight[index * group:(index + 1) * group], preferred_element_type=jnp.float32)
        total = total + lax.optimization_barrier(partial_sum.astype(jnp.bfloat16)).astype(jnp.float32)
    return total.astype(jnp.bfloat16)

def reference(incoming_features, attend_prenormal_scale, probe_matrix, lookup_matrix, content_matrix, forgetting_matrix, result_switch_matrix, forgetting_shift, spike_forget_logarithm, attend_unit_scale, attend_result_matrix, perceptron_scale, content_expand_matrix, switch_expand_matrix, content_kernel, switch_kernel, contract_matrix):

    def lone_context(incoming_tokens):
        weight_fragments, spike_forgetting = incoming_tokens
        normed = row_norm(weight_fragments, attend_prenormal_scale)
        probe_tokens = jnp.dot(normed, probe_matrix, preferred_element_type=jnp.float32).astype(jnp.bfloat16)
        lookup_tokens = jnp.dot(normed, lookup_matrix, preferred_element_type=jnp.float32).astype(jnp.bfloat16)
        content_tokens = jnp.dot(normed, content_matrix, preferred_element_type=jnp.float32).astype(jnp.bfloat16)
        result_switch = jnp.dot(normed, result_switch_matrix, preferred_element_type=jnp.float32).astype(jnp.bfloat16)
        forgetting_raw = jnp.dot(normed, forgetting_matrix, preferred_element_type=jnp.float32) + forgetting_shift
        switched_result = attend_unit_results(probe_tokens, lookup_tokens, content_tokens, result_switch, forgetting_raw, spike_forgetting, attend_unit_scale)
        mix = grouped_product(switched_result, attend_result_matrix)
        middle = (weight_fragments.astype(jnp.float32) + lax.optimization_barrier(mix).astype(jnp.float32)).astype(jnp.bfloat16)
        normed_mid = row_norm(middle, perceptron_scale)
        up_value = jnp.dot(normed_mid, content_expand_matrix, preferred_element_type=jnp.float32).astype(jnp.bfloat16)
        up_gate = jnp.dot(normed_mid, switch_expand_matrix, preferred_element_type=jnp.float32).astype(jnp.bfloat16)
        conv_value = causal_conv(up_value, content_kernel)
        conv_gated = causal_conv(up_gate, switch_kernel)
        hidden = (conv_value * jax.nn.gelu(conv_gated, approximate=True)).astype(jnp.bfloat16)
        ffn = grouped_product(hidden, contract_matrix)
        return (middle.astype(jnp.float32) + lax.optimization_barrier(ffn).astype(jnp.float32)).astype(jnp.bfloat16)
    result_tokens = lax.map(lone_context, (incoming_features.reshape(BATCH_SIZE, CONTEXT_SPAN, EMBED_DIM), spike_forget_logarithm.reshape(BATCH_SIZE, CONTEXT_SPAN, LOOKUP_FEATURES)))
    return result_tokens.reshape(TOKENS, EMBED_DIM)
```

```python
import jax
import jax.numpy as jnp
from jax import lax
from jax.experimental import pallas as pl
from jax.experimental.pallas import tpu as pltpu
from jax.sharding import Mesh
from jax.sharding import PartitionSpec as P

HEAD_K = 32
HEAD_V = 64
BLOCK = 64
SUB = 8
LANES = 128

norm_eps = 1e-06
switch_multiplier = 16.0


def row_norm(content_tokens, gain):
    content_tokens = content_tokens.astype(jnp.float32)
    scaled = content_tokens * lax.rsqrt(
        jnp.mean(content_tokens * content_tokens, axis=-1, keepdims=True) + norm_eps
    )
    return (scaled * gain.astype(jnp.float32)).astype(jnp.bfloat16)


def gated_scan(probe_tokens, lookup_tokens, content_tokens, forgetting_scores):
    length, heads, key_size = probe_tokens.shape
    value_size = content_tokens.shape[-1]
    blocks = length // BLOCK

    def split_blocks(array):
        return array.reshape(blocks, BLOCK, heads, array.shape[-1])

    causal = jnp.arange(BLOCK)[:, None] >= jnp.arange(BLOCK)[None, :]
    highest = lax.Precision.HIGHEST

    def step(state, incoming_tokens):
        query_block, key_block, value_block, decay_block = incoming_tokens
        cumulative = jnp.cumsum(decay_block, axis=0)
        differ = cumulative[:, None] - cumulative[None, :]
        weight = jnp.exp(jnp.where(causal[:, :, None, None], differ, -jnp.inf))
        scores = jnp.einsum("thd,shd,tshd->tsh", query_block, key_block, weight, precision=highest)
        inner = jnp.einsum("tsh,shv->thv", scores, value_block, precision=highest)
        carried = jnp.einsum(
            "thd,hdv->thv", query_block * jnp.exp(cumulative), state, precision=highest
        )
        final = cumulative[-1]
        state = jnp.exp(final)[:, :, None] * state + jnp.einsum(
            "shd,shv->hdv",
            key_block * jnp.exp(final[None] - cumulative),
            value_block,
            precision=highest,
        )
        return (state, inner + carried)

    start_state = jnp.zeros((heads, key_size, value_size), jnp.float32)
    _, result_tokens = lax.scan(
        step,
        start_state,
        (
            split_blocks(probe_tokens),
            split_blocks(lookup_tokens),
            split_blocks(content_tokens),
            split_blocks(forgetting_scores),
        ),
    )
    return result_tokens.reshape(length, heads, value_size)


def attend_unit_results(
    probe_tokens,
    lookup_tokens,
    content_tokens,
    result_switch,
    forgetting_raw,
    spike_forgetting,
    attend_unit_scale,
):
    length = probe_tokens.shape[0]
    heads = probe_tokens.shape[1] // HEAD_K
    forgetting_scores = jax.nn.log_sigmoid(forgetting_raw) / switch_multiplier + spike_forgetting

    def split_heads(array, width):
        return array.astype(jnp.float32).reshape(length, heads, width)

    result_tokens = gated_scan(
        split_heads(probe_tokens, HEAD_K) * HEAD_K ** (-0.5),
        split_heads(lookup_tokens, HEAD_K),
        split_heads(content_tokens, HEAD_V),
        split_heads(forgetting_scores, HEAD_K),
    )
    result_tokens = result_tokens * lax.rsqrt(
        jnp.mean(result_tokens * result_tokens, axis=-1, keepdims=True) + norm_eps
    )
    result_tokens = result_tokens * attend_unit_scale.astype(jnp.float32).reshape(heads, HEAD_V)
    switched_result = result_tokens.reshape(length, heads * HEAD_V) * jax.nn.silu(
        result_switch.astype(jnp.float32)
    )
    return switched_result.astype(jnp.bfloat16)


def causal_conv(content_tokens, taps):
    content_tokens = content_tokens.astype(jnp.float32)
    taps = taps.astype(jnp.float32)
    width = taps.shape[0]
    padded = jnp.pad(content_tokens, ((width - 1, 0), (0, 0)))
    total = jnp.zeros_like(content_tokens)
    for offset in range(width):
        total = total + padded[offset : offset + content_tokens.shape[0]] * taps[offset]
    return total


def general_shards(
    incoming_features,
    attend_prenormal_scale,
    probe_matrix,
    lookup_matrix,
    content_matrix,
    forgetting_matrix,
    result_switch_matrix,
    forgetting_shift,
    spike_forget_logarithm,
    attend_unit_scale,
    attend_result_matrix,
    perceptron_scale,
    content_expand_matrix,
    switch_expand_matrix,
    content_kernel,
    switch_kernel,
    contract_matrix,
):
    whole_in = lax.all_gather(incoming_features, "tp", axis=1, tiled=True)
    columns = row_norm(whole_in, attend_prenormal_scale)
    pieces = tuple(
        lax.all_gather(piece, "fs", axis=0, tiled=True)
        for piece in (
            probe_matrix,
            lookup_matrix,
            content_matrix,
            forgetting_matrix,
            result_switch_matrix,
        )
    )
    query_sum, key_sum, value_sum, decay_sum, gate_sum = tuple(
        (jnp.dot(columns, piece, preferred_element_type=jnp.float32) for piece in pieces)
    )
    switched_result = attend_unit_results(
        query_sum.astype(jnp.bfloat16),
        key_sum.astype(jnp.bfloat16),
        value_sum.astype(jnp.bfloat16),
        gate_sum.astype(jnp.bfloat16),
        decay_sum + forgetting_shift,
        spike_forget_logarithm,
        attend_unit_scale,
    )
    mixer_partial = jnp.dot(
        switched_result,
        lax.all_gather(attend_result_matrix, "fs", axis=1, tiled=True),
        preferred_element_type=jnp.float32,
    )
    mix = lax.psum_scatter(
        mixer_partial.astype(jnp.bfloat16), "tp", scatter_dimension=1, tiled=True
    )
    middle = (
        incoming_features.astype(jnp.float32) + lax.optimization_barrier(mix).astype(jnp.float32)
    ).astype(jnp.bfloat16)
    whole_mid = lax.all_gather(middle, "tp", axis=1, tiled=True)
    columns = row_norm(whole_mid, perceptron_scale)
    pieces = (
        lax.all_gather(content_expand_matrix, "fs", axis=0, tiled=True),
        lax.all_gather(switch_expand_matrix, "fs", axis=0, tiled=True),
    )
    value_total = jnp.dot(columns, pieces[0], preferred_element_type=jnp.float32)
    gate_total = jnp.dot(columns, pieces[1], preferred_element_type=jnp.float32)
    conv_value = causal_conv(value_total.astype(jnp.bfloat16), content_kernel)
    conv_gated = causal_conv(gate_total.astype(jnp.bfloat16), switch_kernel)
    hidden = (conv_value * jax.nn.gelu(conv_gated, approximate=True)).astype(jnp.bfloat16)
    down_partial = jnp.dot(
        hidden,
        lax.all_gather(contract_matrix, "fs", axis=1, tiled=True),
        preferred_element_type=jnp.float32,
    )
    ffn = lax.psum_scatter(down_partial.astype(jnp.bfloat16), "tp", scatter_dimension=1, tiled=True)
    return (middle.astype(jnp.float32) + lax.optimization_barrier(ffn).astype(jnp.float32)).astype(
        jnp.bfloat16
    )


F32 = jnp.float32
BF16 = jnp.bfloat16


def dot(a, b):
    return jnp.dot(a, b, preferred_element_type=F32)


def pack_kernel(
    pos, probe, lookup, content, forget, switch, result, spike, feat,
    own, send, own_spike, to_x, to_y, to_d,
):
    quarter, across = pos[0], pos[1]
    rows = probe.shape[0]
    half = rows // 2
    key_w = probe.shape[1] // 4
    val_w = content.shape[1] // 4
    part = result.shape[0] // 4
    width = feat.shape[1]

    def pack(index, out):
        for q in range(4):

            @pl.when(index == q)
            def _():
                keys = pl.ds(q * key_w, key_w)
                vals = pl.ds(q * val_w, val_w)
                out[0:rows, :] = jnp.concatenate([probe[:, keys], lookup[:, keys]], axis=1)
                out[rows : 2 * rows, :] = content[:, vals]
                out[2 * rows : 3 * rows, :] = switch[:, vals]
                base = 3 * rows
                out[base : base + part, :] = result[q * part : (q + 1) * part, 0:LANES]
                out[base + part : base + 2 * part, :] = result[q * part : (q + 1) * part, LANES:]
                base = base + 2 * part
                decay = forget[:, keys]
                out[base : base + half, :] = jnp.concatenate(
                    [decay[:half], decay[half:]], axis=1
                )

    pack(quarter, own)
    pack(across, send)

    def spikes(index):
        value = spike[:, 0:key_w]
        for q in range(1, 4):
            value = jnp.where(index == q, spike[:, q * key_w : (q + 1) * key_w], value)
        high = value.astype(BF16)
        low = (value - high.astype(F32)).astype(BF16)
        return jnp.concatenate([high, low], axis=1)

    own_spike[...] = spikes(quarter)
    for slot, ref in ((2, to_x), (3, to_y), (4, to_d)):
        ref[:, 0:width] = feat[...]
        ref[:, width:] = spikes(pos[slot])


def attend_kernel(
    pos, mine, theirs, scale, shift, unit, spike_o, spike_x, spike_y, spike_d,
    slot_o, slot_a, slot_b, slot_c, slot_d,
    keep, send,
    w_qk, w_vg, w_f, w_o, qk_s, v_s, g_s, f_s, gated,
):
    core, z, y, last = pos[5], pos[6], pos[7], pos[8]
    rows = slot_o.shape[0] // 2
    chunk = w_qk.shape[0] // 8
    half = chunk // 2
    part = w_o.shape[1]
    span = spike_o.shape[0]
    length = mine.shape[0]
    key_w = f_s.shape[1] // 2

    def fill(zi, source):
        for j in range(2):
            side = y if j == 0 else 1 - y
            shard = zi * 2 + side
            base = j * rows
            at = pl.ds(pl.multiple_of(shard * chunk, chunk), chunk)
            w_qk[at, :] = source(base, chunk)
            w_vg[at, 0:LANES] = source(base + chunk, chunk)
            w_vg[at, LANES:] = source(base + 2 * chunk, chunk)
            base = base + 3 * chunk
            w_o[shard, :, 0:LANES] = source(base, part)
            w_o[shard, :, LANES:] = source(base + part, part)
            base = base + 2 * part
            folded = source(base, half)
            turned = pltpu.roll(folded.astype(F32), key_w, 1).astype(BF16)
            w_f[pl.ds(pl.multiple_of(shard * chunk, chunk), half), :] = folded
            w_f[pl.ds(pl.multiple_of(shard * chunk + half, half), half), :] = turned

    def plain(ref):
        return lambda at, size: ref[at : at + size, :]

    def either(cond, ref, other):
        return lambda at, size: jnp.where(cond, ref[at : at + size, :], other[at : at + size, :])

    first_z = z == 0
    last_z = z == last
    fill(z, plain(slot_o))
    fill(jnp.bitwise_xor(z, 2), plain(slot_c))
    fill(jnp.where(first_z, last, z - 1), either(first_z, slot_d, slot_a))
    fill(jnp.where(last_z, 0, z + 1), either(last_z, slot_d, slot_b))

    def project(s, carry):
        at = pl.ds(pl.multiple_of(s * span, span), span)
        a = mine[at, :].astype(F32)
        b = theirs[at, :].astype(F32)
        total = jnp.sum(a * a, axis=1, keepdims=True) + jnp.sum(b * b, axis=1, keepdims=True)
        inverse = lax.rsqrt(total / scale.shape[1] + norm_eps)
        low = jnp.where(core == 0, a, b)
        high = jnp.where(core == 0, b, a)
        width = a.shape[1]
        normed = jnp.concatenate(
            [
                (low * inverse * scale[:, 0:width].astype(F32)).astype(BF16),
                (high * inverse * scale[:, width:].astype(F32)).astype(BF16),
            ],
            axis=1,
        )
        qk_s[at, :] = dot(normed, w_qk[...]).astype(BF16).astype(F32)
        vg = dot(normed, w_vg[...]).astype(BF16)
        v_s[at, :] = vg[:, 0:LANES]
        g_s[at, :] = vg[:, LANES:]
        f_s[at, :] = dot(normed, w_f[...])
        return carry

    count = length // span
    lax.fori_loop(0, count, project, 0)

    lane = lax.broadcasted_iota(jnp.int32, (span, LANES), 1)
    left = lane < key_w
    row = lax.broadcasted_iota(jnp.int32, (span, LANES), 0)
    lane_head = lax.broadcasted_iota(jnp.int32, (LANES, 2 * LANES), 0) // HEAD_K
    wide_head = lax.broadcasted_iota(jnp.int32, (LANES, 2 * LANES), 1) // HEAD_V
    spread = (lane_head == wide_head).astype(BF16)
    wide_a = lax.broadcasted_iota(jnp.int32, (2 * LANES, 2 * LANES), 0) // HEAD_V
    wide_b = lax.broadcasted_iota(jnp.int32, (2 * LANES, 2 * LANES), 1) // HEAD_V
    same_wide = (wide_a == wide_b).astype(BF16)
    tri = (
        lax.broadcasted_iota(jnp.int32, (span, span), 0)
        >= lax.broadcasted_iota(jnp.int32, (span, span), 1)
    ).astype(BF16)
    heads = LANES // HEAD_K

    def split_dot(a, value):
        one = value.astype(BF16)
        rest = value - one.astype(F32)
        two = rest.astype(BF16)
        three = (rest - two.astype(F32)).astype(BF16)
        return dot(a, one) + dot(a, two) + dot(a, three)

    def pair(p, carry):
        spike_refs = ((spike_o, spike_x), (spike_y, spike_d))
        at_a = pl.ds(pl.multiple_of(p * 2 * span, span), span)
        at_b = pl.ds(pl.multiple_of(p * 2 * span + span, span), span)
        qk_a, qk_b = qk_s[at_a, :], qk_s[at_b, :]
        query = jnp.where(left, qk_a, pltpu.roll(qk_b, key_w, 1)) * HEAD_K ** (-0.5)
        keys = jnp.where(left, pltpu.roll(qk_a, key_w, 1), qk_b)
        v_a, v_b = v_s[at_a, :], v_s[at_b, :]
        value = jnp.concatenate([v_a, v_b], axis=1)
        decay = jnp.where(left, f_s[at_a, :], pltpu.roll(f_s[at_b, :], key_w, 1))
        decay = decay + shift[...]
        spike_a = jnp.where(p == 0, spike_o[...], spike_y[...]).astype(F32)
        spike_b = jnp.where(p == 0, spike_x[...], spike_d[...]).astype(F32)
        spike_a = spike_a + pltpu.roll(spike_a, key_w, 1)
        spike_b = spike_b + pltpu.roll(spike_b, key_w, 1)
        soft = jnp.minimum(decay, 0.0) - jnp.log1p(jnp.exp(-jnp.abs(decay)))
        log_decay = soft / switch_multiplier + jnp.where(left, spike_a, spike_b)
        cum = split_dot(tri, log_decay)

        tiles = span // SUB
        q3 = query.reshape(tiles, SUB, LANES)
        k3 = keys.reshape(tiles, SUB, LANES)
        c3 = cum.reshape(tiles, SUB, LANES)
        valuef = value.astype(F32)
        v3 = valuef.reshape(tiles, SUB, 2 * LANES)
        place = lax.broadcasted_iota(jnp.int32, (tiles, SUB, LANES), 1)
        out = jnp.zeros((span, 2 * LANES), F32)
        for lag in range(SUB):
            if lag == 0:
                term = q3 * k3
                v_lag = v3
            else:
                k_lag = pltpu.roll(k3, lag, 1)
                c_lag = pltpu.roll(c3, lag, 1)
                v_lag = pltpu.roll(v3, lag, 1)
                fall = jnp.exp(jnp.where(place >= lag, c3 - c_lag, -jnp.inf))
                term = q3 * k_lag * fall
            spread_term = dot(term.reshape(span, LANES).astype(BF16), spread)
            out = out + spread_term * v_lag.reshape(span, 2 * LANES)

        size = SUB
        pieces = []
        while size < span:
            blocks = max(span // (2 * size), 1)
            if 2 * size > span:
                second_rows = span - size
            else:
                second_rows = size
            begin = [i * 2 * size for i in range(blocks)]
            q_parts, k_parts, v_parts = [], [], []
            for b0 in begin:
                middle = b0 + size
                ref_row = cum[middle - 1 : middle, :]
                q_parts.append(
                    query[middle : middle + second_rows]
                    * jnp.exp(cum[middle : middle + second_rows] - ref_row)
                )
                k_parts.append(keys[b0:middle] * jnp.exp(ref_row - cum[b0:middle]))
                v_parts.append(value[b0:middle] if size % 16 == 0 else valuef[b0:middle])
            q_all = jnp.concatenate(q_parts, axis=0) if blocks > 1 else q_parts[0]
            k_all = jnp.concatenate(k_parts, axis=0) if blocks > 1 else k_parts[0]
            v_all = (jnp.concatenate(v_parts, axis=0) if blocks > 1 else v_parts[0]).astype(BF16)
            n_q, n_k = q_all.shape[0], k_all.shape[0]
            q_lane = lax.broadcasted_iota(jnp.int32, (n_q, LANES), 1) // HEAD_K
            q_heads = jnp.concatenate(
                [jnp.where(q_lane == h, q_all, 0.0) for h in range(heads)], axis=0
            ).astype(BF16)
            scores = lax.dot_general(
                q_heads, k_all.astype(BF16), (((1,), (1,)), ((), ())), preferred_element_type=F32
            )
            if blocks > 1:
                q_block = (
                    lax.rem(lax.broadcasted_iota(jnp.int32, (heads * n_q, n_k), 0), n_q)
                    // second_rows
                )
                k_block = lax.broadcasted_iota(jnp.int32, (heads * n_q, n_k), 1) // size
                scores = jnp.where(q_block == k_block, scores, 0.0)
            wide = dot(scores.astype(BF16), v_all)
            wide_lane = lax.broadcasted_iota(jnp.int32, (n_q, 2 * LANES), 1) // HEAD_V
            total = wide[0:n_q]
            for h in range(1, heads):
                total = jnp.where(wide_lane == h, wide[h * n_q : (h + 1) * n_q], total)
            zeros = jnp.zeros((size, 2 * LANES), F32)
            full = []
            for i in range(blocks):
                full.append(zeros)
                full.append(total[i * second_rows : (i + 1) * second_rows])
            covered = blocks * size + blocks * second_rows
            if covered < span:
                full.append(jnp.zeros((span - covered, 2 * LANES), F32))
            out = out + jnp.concatenate(full, axis=0)
            size *= 2

        square = out * out
        high = square.astype(BF16)
        low = (square - high.astype(F32)).astype(BF16)
        mean = (dot(high, same_wide) + dot(low, same_wide)) / HEAD_V
        out = out * lax.rsqrt(mean + norm_eps)
        gate = jnp.concatenate([g_s[at_a, :], g_s[at_b, :]], axis=1).astype(F32)
        gain = unit[...].astype(F32)
        out = out * jnp.concatenate([gain, gain], axis=1)
        out = out * (gate / (1.0 + jnp.exp(-gate)))
        gated[at_a, :] = out[:, 0:LANES].astype(BF16)
        gated[at_b, :] = out[:, LANES:].astype(BF16)
        return carry

    lax.fori_loop(0, count // 2, pair, 0)
    mix_out(core, gated, w_o, keep, send, span)


def mix_out(core, left, weights, keep, send, span):
    shards = weights.shape[0]
    width = weights.shape[2]
    for h in range(2):
        for f in range(shards // 2):
            w = weights[h * (shards // 2) + f]
            value = dot(left[...], w).astype(BF16)
            cols = slice(f * width, (f + 1) * width)

            @pl.when(core == h)
            def _():
                keep[:, cols] = value

            @pl.when(core != h)
            def _():
                send[:, cols] = value


def expand_kernel(
    pos, mine, theirs, scale, taps_v, taps_g, slot_o, slot_a, slot_b, slot_c, slot_d,
    hidden, w_up,
):
    core, z, y, last = pos[5], pos[6], pos[7], pos[8]
    chunk = slot_o.shape[0] // 2
    span = hidden.shape[0] // 4
    width = hidden.shape[1]

    def fill(zi, source):
        for j in range(2):
            side = y if j == 0 else 1 - y
            at = pl.ds(pl.multiple_of((zi * 2 + side) * chunk, chunk), chunk)
            w_up[at, :] = source(j * chunk, chunk)

    def plain(ref):
        return lambda at, size: ref[at : at + size, :]

    def either(cond, ref, other):
        return lambda at, size: jnp.where(cond, ref[at : at + size, :], other[at : at + size, :])

    first_z = z == 0
    last_z = z == last
    fill(z, plain(slot_o))
    fill(jnp.bitwise_xor(z, 2), plain(slot_c))
    fill(jnp.where(first_z, last, z - 1), either(first_z, slot_d, slot_a))
    fill(jnp.where(last_z, 0, z + 1), either(last_z, slot_d, slot_b))

    def conv(value, taps):
        taps = taps.astype(F32)
        row = lax.broadcasted_iota(jnp.int32, value.shape, 0)
        total = value * taps[2:3]
        total = total + jnp.where(row >= 1, pltpu.roll(value, 1, 0), 0.0) * taps[1:2]
        return total + jnp.where(row >= 2, pltpu.roll(value, 2, 0), 0.0) * taps[0:1]

    def sequence(s, carry):
        at = pl.ds(pl.multiple_of(s * span, span), span)
        a = mine[at, :].astype(F32)
        b = theirs[at, :].astype(F32)
        total = jnp.sum(a * a, axis=1, keepdims=True) + jnp.sum(b * b, axis=1, keepdims=True)
        inverse = lax.rsqrt(total / scale.shape[1] + norm_eps)
        low = jnp.where(core == 0, a, b)
        high = jnp.where(core == 0, b, a)
        half = a.shape[1]
        normed = jnp.concatenate(
            [
                (low * inverse * scale[:, 0:half].astype(F32)).astype(BF16),
                (high * inverse * scale[:, half:].astype(F32)).astype(BF16),
            ],
            axis=1,
        )
        value = dot(normed, w_up[:, 0:width]).astype(BF16).astype(F32)
        gate = dot(normed, w_up[:, width:]).astype(BF16).astype(F32)
        value = conv(value, taps_v[...])
        gate = conv(gate, taps_g[...])
        hidden[at, :] = (value * jax.nn.gelu(gate, approximate=True)).astype(BF16)
        return carry

    lax.fori_loop(0, 4, sequence, 0)


def contract_kernel(pos, hidden, slot_o, slot_a, slot_b, slot_c, slot_d, keep, send, w_down):
    core, z, y, last = pos[5], pos[6], pos[7], pos[8]
    chunk = slot_o.shape[0] // 2

    def fill(zi, source):
        for j in range(2):
            side = y if j == 0 else 1 - y
            w_down[zi * 2 + side] = source(j * chunk, chunk)

    def plain(ref):
        return lambda at, size: ref[at : at + size, :]

    def either(cond, ref, other):
        return lambda at, size: jnp.where(cond, ref[at : at + size, :], other[at : at + size, :])

    first_z = z == 0
    last_z = z == last
    fill(z, plain(slot_o))
    fill(jnp.bitwise_xor(z, 2), plain(slot_c))
    fill(jnp.where(first_z, last, z - 1), either(first_z, slot_d, slot_a))
    fill(jnp.where(last_z, 0, z + 1), either(last_z, slot_d, slot_b))
    mix_out(core, hidden, w_down, keep, send, hidden.shape[0] // 4)


def call(kernel, outs, args, scratch=(), name=None, flops=0):
    in_specs = [pl.BlockSpec(memory_space=pltpu.SMEM)]
    in_specs += [pl.BlockSpec(memory_space=pltpu.VMEM)] * (len(args) - 1)
    return pl.pallas_call(
        kernel,
        out_shape=[jax.ShapeDtypeStruct(*o) for o in outs],
        in_specs=in_specs,
        out_specs=[pl.BlockSpec(memory_space=pltpu.VMEM)] * len(outs),
        scratch_shapes=list(scratch),
        cost_estimate=pl.CostEstimate(flops=flops, bytes_accessed=1 << 20, transcendentals=0),
        compiler_params=pltpu.CompilerParams(vmem_limit_bytes=56 << 20),
        name=name,
    )(*args)


def plane_shards(sizes):
    n_x, n_z, n_y, n_c = sizes
    axes = ("rep", "z", "y", "tp")

    def pairs(move):
        found = []
        for x in range(n_x):
            for z in range(n_z):
                for y in range(n_y):
                    for c in range(n_c):
                        to = move(x, z, y, c)
                        if to is not None:
                            a = ((x * n_z + z) * n_y + y) * n_c + c
                            b = ((to[0] * n_z + to[1]) * n_y + to[2]) * n_c + to[3]
                            found.append((a, b))
        return found

    over_x = pairs(lambda x, z, y, c: (1 - x, z, y, c))
    over_y = pairs(lambda x, z, y, c: (x, z, 1 - y, c))
    over_d = pairs(lambda x, z, y, c: (1 - x, z, 1 - y, c))
    over_c = pairs(lambda x, z, y, c: (x, z, y, 1 - c))
    up_z = pairs(lambda x, z, y, c: (x, z + 1, y, c) if z + 1 < n_z else None)
    down_z = pairs(lambda x, z, y, c: (x, z - 1, y, c) if z > 0 else None)
    skip_z = pairs(lambda x, z, y, c: (x, (z + 2) % n_z, y, c))
    ends_z = pairs(
        lambda x, z, y, c: (x, 3, y, c) if z == 2 else ((x, 0, y, c) if z == 1 else None)
    )

    def move(value, perm):
        return lax.ppermute(value, axes, perm)

    def gather(own, received):
        slot = jnp.concatenate([own, received], axis=0)
        a = move(slot, up_z)
        b = move(slot, down_z)
        c = move(slot, skip_z)
        d = move(c, ends_z)
        return slot, a, b, c, d

    def shards(
        incoming_features,
        attend_prenormal_scale,
        probe_matrix,
        lookup_matrix,
        content_matrix,
        forgetting_matrix,
        result_switch_matrix,
        forgetting_shift,
        spike_forget_logarithm,
        attend_unit_scale,
        attend_result_matrix,
        perceptron_scale,
        content_expand_matrix,
        switch_expand_matrix,
        content_kernel,
        switch_kernel,
        contract_matrix,
    ):
        x, z, y, c = (lax.axis_index(axis) for axis in axes)
        quarter = 2 * x + y
        pos = jnp.stack(
            [
                quarter,
                2 * x + (1 - y),
                2 * (1 - x) + y,
                2 * x + (1 - y),
                2 * (1 - x) + (1 - y),
                c,
                z,
                y,
                jnp.int32(n_z - 1),
            ]
        ).astype(jnp.int32)
        span, width = incoming_features.shape
        embed = width * n_c
        chunk = probe_matrix.shape[0]
        part = attend_result_matrix.shape[0] // 4
        pack_rows = 3 * chunk + 2 * part + chunk // 2
        own, send, spike_o, to_x, to_y, to_d = call(
            pack_kernel,
            [
                ((pack_rows, LANES), BF16),
                ((pack_rows, LANES), BF16),
                ((span, LANES), BF16),
            ]
            + [((span, width + LANES), BF16)] * 3,
            (
                pos,
                probe_matrix,
                lookup_matrix,
                content_matrix,
                forgetting_matrix,
                result_switch_matrix,
                attend_result_matrix,
                spike_forget_logarithm,
                incoming_features,
            ),
            name="pack",
        )
        attn = gather(own, move(send, over_y))
        from_x = move(to_x, over_x)
        from_y = move(to_y, over_y)
        from_d = move(to_d, over_d)

        ff = content_expand_matrix.shape[1] // 4

        def up_part(index):
            return jnp.concatenate(
                [
                    lax.dynamic_slice_in_dim(content_expand_matrix, index * ff, ff, 1),
                    lax.dynamic_slice_in_dim(switch_expand_matrix, index * ff, ff, 1),
                ],
                axis=1,
            )

        def down_part(index):
            return lax.dynamic_slice_in_dim(contract_matrix, index * ff, ff, 0)

        across = 2 * x + (1 - y)
        up = gather(up_part(quarter), move(up_part(across), over_y))
        down = gather(down_part(quarter), move(down_part(across), over_y))

        def halves(blocks):
            mine = jnp.concatenate(blocks, axis=0)
            return mine, move(mine, over_c)

        def reduce(keep, other):
            total = (keep.astype(F32) + other.astype(F32)).astype(BF16)
            blocks = [total[i * span : (i + 1) * span] for i in range(4)]
            return (
                blocks[0],
                move(blocks[1], over_x),
                move(blocks[2], over_y),
                move(blocks[3], over_d),
            )

        def add_up(base, parts):
            total = parts[0].astype(F32)
            for part_ in parts[1:]:
                total = total + part_.astype(F32)
            return (base.astype(F32) + total.astype(BF16).astype(F32)).astype(BF16)

        tokens = 4 * span
        mine, theirs = halves(
            [incoming_features] + [value[:, :width] for value in (from_x, from_y, from_d)]
        )
        key_w = forgetting_shift.shape[0] // 4
        val_w = attend_unit_scale.shape[0] // 4
        shift = lax.dynamic_slice_in_dim(forgetting_shift, quarter * key_w, key_w, 0)
        shift = jnp.concatenate([shift, shift]).reshape(1, LANES)
        unit = lax.dynamic_slice_in_dim(attend_unit_scale, quarter * val_w, val_w, 0)
        keep, other = call(
            attend_kernel,
            [((tokens, width), BF16)] * 2,
            (
                pos,
                mine,
                theirs,
                attend_prenormal_scale.reshape(1, embed),
                shift,
                unit.reshape(1, val_w),
                spike_o,
                from_x[:, width:],
                from_y[:, width:],
                from_d[:, width:],
            )
            + attn,
            scratch=[
                pltpu.VMEM((embed, LANES), BF16),
                pltpu.VMEM((embed, 2 * LANES), BF16),
                pltpu.VMEM((embed, LANES), BF16),
                pltpu.VMEM((8, part, embed // 8), BF16),
                pltpu.VMEM((tokens, LANES), F32),
                pltpu.VMEM((tokens, LANES), BF16),
                pltpu.VMEM((tokens, LANES), BF16),
                pltpu.VMEM((tokens, LANES), F32),
                pltpu.VMEM((tokens, LANES), BF16),
            ],
            name="attend",
            flops=10**10,
        )
        middle = add_up(incoming_features, reduce(keep, move(other, over_c)))
        mine, theirs = halves(
            [middle, move(middle, over_x), move(middle, over_y), move(middle, over_d)]
        )
        taps_v = lax.dynamic_slice_in_dim(content_kernel, quarter * ff, ff, 1)
        taps_g = lax.dynamic_slice_in_dim(switch_kernel, quarter * ff, ff, 1)
        (hidden,) = call(
            expand_kernel,
            [((tokens, ff), BF16)],
            (pos, mine, theirs, perceptron_scale.reshape(1, embed), taps_v, taps_g) + up,
            scratch=[pltpu.VMEM((embed, 2 * ff), BF16)],
            name="expand",
            flops=10**10,
        )
        keep, other = call(
            contract_kernel,
            [((tokens, width), BF16)] * 2,
            (pos, hidden) + down,
            scratch=[pltpu.VMEM((8, ff, embed // 8), BF16)],
            name="contract",
            flops=10**10,
        )
        return add_up(middle, reduce(keep, move(other, over_c)))

    return shards


def plane_sizes(mesh):
    if tuple(mesh.axis_names) != ("rep", "fs", "tp"):
        return None
    n_x, n_fs, n_c = (mesh.shape[axis] for axis in ("rep", "fs", "tp"))
    if n_x != 2 or n_c != 2 or n_fs % 2 or n_fs // 2 != 4:
        return None
    return (n_x, n_fs // 2, 2, n_c)


def solution(mesh):
    sizes = plane_sizes(mesh)
    if sizes is None:
        body, seq = general_shards, ("rep", "fs")
        weight = ("fs",)
        used = mesh
    else:
        body, seq = plane_shards(sizes), ("rep", "z", "y")
        weight = ("z", "y")
        used = Mesh(mesh.devices.reshape(sizes), ("rep", "z", "y", "tp"))
    placed = (
        P(seq, "tp"),
        P(),
        P(weight, "tp"),
        P(weight, "tp"),
        P(weight, "tp"),
        P(weight, "tp"),
        P(weight, "tp"),
        P("tp"),
        P(seq, "tp"),
        P("tp"),
        P("tp", weight),
        P(),
        P(weight, "tp"),
        P(weight, "tp"),
        P(None, "tp"),
        P(None, "tp"),
        P("tp", weight),
    )
    return jax.shard_map(body, mesh=used, in_specs=placed, out_specs=P(seq, "tp"), check_vma=False)
```

```python
import jax
import jax.numpy as jnp
from jax import lax
from jax.experimental import pallas as pl
from jax.experimental.pallas import tpu as pltpu
from jax.sharding import Mesh
from jax.sharding import PartitionSpec as P


HEAD_K = 32
HEAD_V = 64
BLOCK = 64
SUB = 8
LANES = 128

norm_eps = 1e-06
switch_multiplier = 16.0


def row_norm(content_tokens, gain):
    content_tokens = content_tokens.astype(jnp.float32)
    scaled = content_tokens * lax.rsqrt(
        jnp.mean(content_tokens * content_tokens, axis=-1, keepdims=True) + norm_eps
    )
    return (scaled * gain.astype(jnp.float32)).astype(jnp.bfloat16)


def gated_scan(probe_tokens, lookup_tokens, content_tokens, forgetting_scores):
    length, heads, key_size = probe_tokens.shape
    value_size = content_tokens.shape[-1]
    blocks = length // BLOCK

    def split_blocks(array):
        return array.reshape(blocks, BLOCK, heads, array.shape[-1])

    causal = jnp.arange(BLOCK)[:, None] >= jnp.arange(BLOCK)[None, :]
    highest = lax.Precision.HIGHEST

    def step(state, incoming_tokens):
        query_block, key_block, value_block, decay_block = incoming_tokens
        cumulative = jnp.cumsum(decay_block, axis=0)
        differ = cumulative[:, None] - cumulative[None, :]
        weight = jnp.exp(jnp.where(causal[:, :, None, None], differ, -jnp.inf))
        scores = jnp.einsum("thd,shd,tshd->tsh", query_block, key_block, weight, precision=highest)
        inner = jnp.einsum("tsh,shv->thv", scores, value_block, precision=highest)
        carried = jnp.einsum(
            "thd,hdv->thv", query_block * jnp.exp(cumulative), state, precision=highest
        )
        final = cumulative[-1]
        state = jnp.exp(final)[:, :, None] * state + jnp.einsum(
            "shd,shv->hdv",
            key_block * jnp.exp(final[None] - cumulative),
            value_block,
            precision=highest,
        )
        return (state, inner + carried)

    start_state = jnp.zeros((heads, key_size, value_size), jnp.float32)
    _, result_tokens = lax.scan(
        step,
        start_state,
        (
            split_blocks(probe_tokens),
            split_blocks(lookup_tokens),
            split_blocks(content_tokens),
            split_blocks(forgetting_scores),
        ),
    )
    return result_tokens.reshape(length, heads, value_size)


def attend_unit_results(
    probe_tokens,
    lookup_tokens,
    content_tokens,
    result_switch,
    forgetting_raw,
    spike_forgetting,
    attend_unit_scale,
):
    length = probe_tokens.shape[0]
    heads = probe_tokens.shape[1] // HEAD_K
    forgetting_scores = jax.nn.log_sigmoid(forgetting_raw) / switch_multiplier + spike_forgetting

    def split_heads(array, width):
        return array.astype(jnp.float32).reshape(length, heads, width)

    result_tokens = gated_scan(
        split_heads(probe_tokens, HEAD_K) * HEAD_K ** (-0.5),
        split_heads(lookup_tokens, HEAD_K),
        split_heads(content_tokens, HEAD_V),
        split_heads(forgetting_scores, HEAD_K),
    )
    result_tokens = result_tokens * lax.rsqrt(
        jnp.mean(result_tokens * result_tokens, axis=-1, keepdims=True) + norm_eps
    )
    result_tokens = result_tokens * attend_unit_scale.astype(jnp.float32).reshape(heads, HEAD_V)
    switched_result = result_tokens.reshape(length, heads * HEAD_V) * jax.nn.silu(
        result_switch.astype(jnp.float32)
    )
    return switched_result.astype(jnp.bfloat16)


def causal_conv(content_tokens, taps):
    content_tokens = content_tokens.astype(jnp.float32)
    taps = taps.astype(jnp.float32)
    width = taps.shape[0]
    padded = jnp.pad(content_tokens, ((width - 1, 0), (0, 0)))
    total = jnp.zeros_like(content_tokens)
    for offset in range(width):
        total = total + padded[offset : offset + content_tokens.shape[0]] * taps[offset]
    return total


def general_shards(
    incoming_features,
    attend_prenormal_scale,
    probe_matrix,
    lookup_matrix,
    content_matrix,
    forgetting_matrix,
    result_switch_matrix,
    forgetting_shift,
    spike_forget_logarithm,
    attend_unit_scale,
    attend_result_matrix,
    perceptron_scale,
    content_expand_matrix,
    switch_expand_matrix,
    content_kernel,
    switch_kernel,
    contract_matrix,
):
    whole_in = lax.all_gather(incoming_features, "tp", axis=1, tiled=True)
    columns = row_norm(whole_in, attend_prenormal_scale)
    pieces = tuple(
        lax.all_gather(piece, "fs", axis=0, tiled=True)
        for piece in (
            probe_matrix,
            lookup_matrix,
            content_matrix,
            forgetting_matrix,
            result_switch_matrix,
        )
    )
    query_sum, key_sum, value_sum, decay_sum, gate_sum = tuple(
        (jnp.dot(columns, piece, preferred_element_type=jnp.float32) for piece in pieces)
    )
    switched_result = attend_unit_results(
        query_sum.astype(jnp.bfloat16),
        key_sum.astype(jnp.bfloat16),
        value_sum.astype(jnp.bfloat16),
        gate_sum.astype(jnp.bfloat16),
        decay_sum + forgetting_shift,
        spike_forget_logarithm,
        attend_unit_scale,
    )
    mixer_partial = jnp.dot(
        switched_result,
        lax.all_gather(attend_result_matrix, "fs", axis=1, tiled=True),
        preferred_element_type=jnp.float32,
    )
    mix = lax.psum_scatter(
        mixer_partial.astype(jnp.bfloat16), "tp", scatter_dimension=1, tiled=True
    )
    middle = (
        incoming_features.astype(jnp.float32) + lax.optimization_barrier(mix).astype(jnp.float32)
    ).astype(jnp.bfloat16)
    whole_mid = lax.all_gather(middle, "tp", axis=1, tiled=True)
    columns = row_norm(whole_mid, perceptron_scale)
    pieces = (
        lax.all_gather(content_expand_matrix, "fs", axis=0, tiled=True),
        lax.all_gather(switch_expand_matrix, "fs", axis=0, tiled=True),
    )
    value_total = jnp.dot(columns, pieces[0], preferred_element_type=jnp.float32)
    gate_total = jnp.dot(columns, pieces[1], preferred_element_type=jnp.float32)
    conv_value = causal_conv(value_total.astype(jnp.bfloat16), content_kernel)
    conv_gated = causal_conv(gate_total.astype(jnp.bfloat16), switch_kernel)
    hidden = (conv_value * jax.nn.gelu(conv_gated, approximate=True)).astype(jnp.bfloat16)
    down_partial = jnp.dot(
        hidden,
        lax.all_gather(contract_matrix, "fs", axis=1, tiled=True),
        preferred_element_type=jnp.float32,
    )
    ffn = lax.psum_scatter(down_partial.astype(jnp.bfloat16), "tp", scatter_dimension=1, tiled=True)
    return (middle.astype(jnp.float32) + lax.optimization_barrier(ffn).astype(jnp.float32)).astype(
        jnp.bfloat16
    )


F32 = jnp.float32
BF16 = jnp.bfloat16


def dot(a, b):
    return jnp.dot(a, b, preferred_element_type=F32)


def pack_kernel(pos, probe, lookup, content, forget, switch, result, own, send):
    quarter, across = pos[0], pos[1]
    rows = probe.shape[0]
    half = rows // 2
    key_w = probe.shape[1] // 4
    val_w = content.shape[1] // 4
    part = result.shape[0] // 4

    def pack(index, out):
        for q in range(4):

            @pl.when(index == q)
            def _():
                keys = pl.ds(q * key_w, key_w)
                vals = pl.ds(q * val_w, val_w)
                out[0:rows, :] = jnp.concatenate([probe[:, keys], lookup[:, keys]], axis=1)
                out[rows : 2 * rows, :] = content[:, vals]
                out[2 * rows : 3 * rows, :] = switch[:, vals]
                base = 3 * rows
                out[base : base + part, :] = result[q * part : (q + 1) * part, 0:LANES]
                out[base + part : base + 2 * part, :] = result[q * part : (q + 1) * part, LANES:]
                base = base + 2 * part
                decay = forget[:, keys]
                out[base : base + half, :] = jnp.concatenate(
                    [decay[:half], decay[half:]], axis=1
                )

    pack(across, send)
    pack(quarter, own)


def input_kernel(pos, spike, feat, own_spike, to_x, to_y, to_d):
    key_w = spike.shape[1] // 4
    width = feat.shape[1]

    def spikes(index):
        value = spike[:, 0:key_w]
        for q in range(1, 4):
            value = jnp.where(index == q, spike[:, q * key_w : (q + 1) * key_w], value)
        high = value.astype(BF16)
        low = (value - high.astype(F32)).astype(BF16)
        return jnp.concatenate([high, low], axis=1)

    own_spike[...] = spikes(pos[0])
    for slot, ref in ((2, to_x), (3, to_y), (4, to_d)):
        ref[:, 0:width] = feat[...]
        ref[:, width:] = spikes(pos[slot])


def copy_from(choices, sem, dst, cut):
    for cond, ref in choices:
        copy = pltpu.make_async_copy(cut(ref), dst, sem)
        if cond is None:
            copy.start()
        else:
            pl.when(cond)(copy.start)


def blocks_of(pos, slots):
    slot_o, slot_r1, slot_l1, slot_r2, slot_l2, slot_r3, slot_l3 = slots
    z, last = pos[6], pos[8]
    low = z < 2
    first_z = z == 0
    last_z = z == last
    return (
        (z, ((None, slot_o),)),
        (jnp.bitwise_xor(z, 2), ((low, slot_l2), (jnp.logical_not(low), slot_r2))),
        (
            jnp.where(first_z, last, z - 1),
            ((first_z, slot_l3), (jnp.logical_not(first_z), slot_r1)),
        ),
        (
            jnp.where(last_z, 0, z + 1),
            ((last_z, slot_r3), (jnp.logical_not(last_z), slot_l1)),
        ),
    )


def attend_kernel(
    pos, mine, theirs, scale, shift, unit, spike_o, spike_x, spike_y, spike_d,
    slot_o, slot_r1, slot_l1, slot_r2, slot_l2, slot_r3, slot_l3,
    keep, send,
    w_qk, w_vg, w_f, w_o, folded, qk_s, v_s, g_s, f_s, gated, sems,
):
    core, y = pos[5], pos[7]
    rows = slot_o.shape[0] // 2
    chunk = w_qk.shape[0] // 8
    half = chunk // 2
    part = w_o.shape[1]
    span = spike_o.shape[0]
    length, width = mine.shape
    key_w = f_s.shape[1] // 2

    slots = (slot_o, slot_r1, slot_l1, slot_r2, slot_l2, slot_r3, slot_l3)
    waits = []
    for index, (zi, choices) in enumerate(blocks_of(pos, slots)):
        for j in range(2):
            shard = zi * 2 + (y if j == 0 else 1 - y)
            at = pl.ds(pl.multiple_of(shard * chunk, chunk), chunk)
            base = j * rows
            targets = (
                (w_qk.at[at, :], chunk),
                (w_vg.at[at, 0:LANES], chunk),
                (w_vg.at[at, LANES : 2 * LANES], chunk),
                (w_o.at[shard, :, 0:LANES], part),
                (w_o.at[shard, :, LANES : 2 * LANES], part),
                (folded.at[shard], half),
            )
            for k, (dst, size) in enumerate(targets):
                sem = sems.at[index * 12 + j * 6 + k]
                copy_from(choices, sem, dst, lambda ref, b=base, n=size: ref.at[pl.ds(b, n), :])
                waits.append((slot_o.at[pl.ds(base, size), :], dst, sem))
                base += size
    for source, dst, sem in waits:
        pltpu.make_async_copy(source, dst, sem).wait()
    for shard in range(8):
        w_f[shard * chunk : shard * chunk + half, :] = folded[shard]
        w_f[shard * chunk + half : (shard + 1) * chunk, :] = pltpu.roll(
            folded[shard].astype(F32), key_w, 1
        ).astype(BF16)

    def project(s, carry):
        at = pl.ds(pl.multiple_of(s * span, span), span)
        a = mine[at, :].astype(F32)
        b = theirs[at, :].astype(F32)
        total = jnp.sum(a * a, axis=1, keepdims=True) + jnp.sum(b * b, axis=1, keepdims=True)
        inverse = lax.rsqrt(total / scale.shape[1] + norm_eps)
        low = jnp.where(core == 0, a, b)
        high = jnp.where(core == 0, b, a)
        width = a.shape[1]
        normed = jnp.concatenate(
            [
                (low * inverse * scale[:, 0:width].astype(F32)).astype(BF16),
                (high * inverse * scale[:, width:].astype(F32)).astype(BF16),
            ],
            axis=1,
        )
        qk_s[at, :] = dot(normed, w_qk[...]).astype(BF16).astype(F32)
        vg = dot(normed, w_vg[...]).astype(BF16)
        v_s[at, :] = vg[:, 0:LANES]
        g_s[at, :] = vg[:, LANES:]
        f_s[at, :] = dot(normed, w_f[...])
        return carry

    count = length // span
    lax.fori_loop(0, count, project, 0)

    lane = lax.broadcasted_iota(jnp.int32, (span, LANES), 1)
    left = lane < key_w
    row = lax.broadcasted_iota(jnp.int32, (span, LANES), 0)
    lane_head = lax.broadcasted_iota(jnp.int32, (LANES, 2 * LANES), 0) // HEAD_K
    wide_head = lax.broadcasted_iota(jnp.int32, (LANES, 2 * LANES), 1) // HEAD_V
    spread = (lane_head == wide_head).astype(BF16)
    wide_a = lax.broadcasted_iota(jnp.int32, (2 * LANES, 2 * LANES), 0) // HEAD_V
    wide_b = lax.broadcasted_iota(jnp.int32, (2 * LANES, 2 * LANES), 1) // HEAD_V
    same_wide = (wide_a == wide_b).astype(BF16)
    tri = (
        lax.broadcasted_iota(jnp.int32, (span, span), 0)
        >= lax.broadcasted_iota(jnp.int32, (span, span), 1)
    ).astype(BF16)
    heads = LANES // HEAD_K

    def split_dot(a, value):
        one = value.astype(BF16)
        rest = value - one.astype(F32)
        two = rest.astype(BF16)
        three = (rest - two.astype(F32)).astype(BF16)
        return dot(a, one) + dot(a, two) + dot(a, three)

    def pair(p, carry):
        at_a = pl.ds(pl.multiple_of(p * 2 * span, span), span)
        at_b = pl.ds(pl.multiple_of(p * 2 * span + span, span), span)
        qk_a, qk_b = qk_s[at_a, :], qk_s[at_b, :]
        query = jnp.where(left, qk_a, pltpu.roll(qk_b, key_w, 1)) * HEAD_K ** (-0.5)
        keys = jnp.where(left, pltpu.roll(qk_a, key_w, 1), qk_b)
        v_a, v_b = v_s[at_a, :], v_s[at_b, :]
        value = jnp.concatenate([v_a, v_b], axis=1)
        decay = jnp.where(left, f_s[at_a, :], pltpu.roll(f_s[at_b, :], key_w, 1))
        decay = decay + shift[...]
        spike_a = jnp.where(p == 0, spike_o[...], spike_y[:, width:]).astype(F32)
        spike_b = jnp.where(p == 0, spike_x[:, width:], spike_d[:, width:]).astype(F32)
        spike_a = spike_a + pltpu.roll(spike_a, key_w, 1)
        spike_b = spike_b + pltpu.roll(spike_b, key_w, 1)
        soft = jnp.minimum(decay, 0.0) - jnp.log1p(jnp.exp(-jnp.abs(decay)))
        log_decay = soft / switch_multiplier + jnp.where(left, spike_a, spike_b)
        cum = split_dot(tri, log_decay)

        tiles = span // SUB
        q3 = query.reshape(tiles, SUB, LANES)
        k3 = keys.reshape(tiles, SUB, LANES)
        c3 = cum.reshape(tiles, SUB, LANES)
        valuef = value.astype(F32)
        v3 = valuef.reshape(tiles, SUB, 2 * LANES)
        place = lax.broadcasted_iota(jnp.int32, (tiles, SUB, LANES), 1)
        out = jnp.zeros((span, 2 * LANES), F32)
        for lag in range(SUB):
            if lag == 0:
                term = q3 * k3
                v_lag = v3
            else:
                k_lag = pltpu.roll(k3, lag, 1)
                c_lag = pltpu.roll(c3, lag, 1)
                v_lag = pltpu.roll(v3, lag, 1)
                fall = jnp.exp(jnp.where(place >= lag, c3 - c_lag, -jnp.inf))
                term = q3 * k_lag * fall
            spread_term = dot(term.reshape(span, LANES).astype(BF16), spread)
            out = out + spread_term * v_lag.reshape(span, 2 * LANES)

        size = SUB
        while size < span:
            blocks = max(span // (2 * size), 1)
            if 2 * size > span:
                second_rows = span - size
            else:
                second_rows = size
            begin = [i * 2 * size for i in range(blocks)]
            q_parts, k_parts, v_parts = [], [], []
            for b0 in begin:
                middle = b0 + size
                ref_row = cum[middle - 1 : middle, :]
                q_parts.append(
                    query[middle : middle + second_rows]
                    * jnp.exp(cum[middle : middle + second_rows] - ref_row)
                )
                k_parts.append(keys[b0:middle] * jnp.exp(ref_row - cum[b0:middle]))
                v_parts.append(value[b0:middle] if size % 16 == 0 else valuef[b0:middle])
            q_all = jnp.concatenate(q_parts, axis=0) if blocks > 1 else q_parts[0]
            k_all = jnp.concatenate(k_parts, axis=0) if blocks > 1 else k_parts[0]
            v_all = (jnp.concatenate(v_parts, axis=0) if blocks > 1 else v_parts[0]).astype(BF16)
            n_q, n_k = q_all.shape[0], k_all.shape[0]
            q_lane = lax.broadcasted_iota(jnp.int32, (n_q, LANES), 1) // HEAD_K
            q_heads = jnp.concatenate(
                [jnp.where(q_lane == h, q_all, 0.0) for h in range(heads)], axis=0
            ).astype(BF16)
            scores = lax.dot_general(
                q_heads, k_all.astype(BF16), (((1,), (1,)), ((), ())), preferred_element_type=F32
            )
            if blocks > 1:
                q_block = (
                    lax.rem(lax.broadcasted_iota(jnp.int32, (heads * n_q, n_k), 0), n_q)
                    // second_rows
                )
                k_block = lax.broadcasted_iota(jnp.int32, (heads * n_q, n_k), 1) // size
                scores = jnp.where(q_block == k_block, scores, 0.0)
            wide = dot(scores.astype(BF16), v_all)
            wide_lane = lax.broadcasted_iota(jnp.int32, (n_q, 2 * LANES), 1) // HEAD_V
            total = wide[0:n_q]
            for h in range(1, heads):
                total = jnp.where(wide_lane == h, wide[h * n_q : (h + 1) * n_q], total)
            zeros = jnp.zeros((size, 2 * LANES), F32)
            full = []
            for i in range(blocks):
                full.append(zeros)
                full.append(total[i * second_rows : (i + 1) * second_rows])
            covered = blocks * size + blocks * second_rows
            if covered < span:
                full.append(jnp.zeros((span - covered, 2 * LANES), F32))
            out = out + jnp.concatenate(full, axis=0)
            size *= 2

        square = out * out
        high = square.astype(BF16)
        low = (square - high.astype(F32)).astype(BF16)
        mean = (dot(high, same_wide) + dot(low, same_wide)) / HEAD_V
        out = out * lax.rsqrt(mean + norm_eps)
        gate = jnp.concatenate([g_s[at_a, :], g_s[at_b, :]], axis=1).astype(F32)
        gain = unit[...].astype(F32)
        out = out * jnp.concatenate([gain, gain], axis=1)
        out = out * (gate / (1.0 + jnp.exp(-gate)))
        gated[at_a, :] = out[:, 0:LANES].astype(BF16)
        gated[at_b, :] = out[:, LANES:].astype(BF16)
        return carry

    lax.fori_loop(0, count // 2, pair, 0)
    mix_out(core, gated, w_o, keep, send)


def mix_out(core, left, weights, keep, send):
    shards = weights.shape[0]
    width = weights.shape[2]
    for h in range(2):
        for f in range(shards // 2):
            w = weights[h * (shards // 2) + f]
            value = dot(left[...], w).astype(BF16)
            cols = slice(f * width, (f + 1) * width)

            @pl.when(core == h)
            def _():
                keep[:, cols] = value

            @pl.when(core != h)
            def _():
                send[:, cols] = value


def expand_kernel(
    pos, mine, theirs, scale, taps_v, taps_g,
    slot_o, slot_r1, slot_l1, slot_r2, slot_l2, slot_r3, slot_l3,
    hidden, w_up, sems,
):
    core, y = pos[5], pos[7]
    chunk = slot_o.shape[0] // 2
    span = hidden.shape[0] // 4
    width = hidden.shape[1]

    slots = (slot_o, slot_r1, slot_l1, slot_r2, slot_l2, slot_r3, slot_l3)
    waits = []
    for index, (zi, choices) in enumerate(blocks_of(pos, slots)):
        for j in range(2):
            side = y if j == 0 else 1 - y
            dst = w_up.at[pl.ds(pl.multiple_of((zi * 2 + side) * chunk, chunk), chunk), :]
            sem = sems.at[index * 2 + j]
            copy_from(choices, sem, dst, lambda ref, b=j * chunk: ref.at[pl.ds(b, chunk), :])
            waits.append((slot_o.at[pl.ds(j * chunk, chunk), :], dst, sem))
    for source, dst, sem in waits:
        pltpu.make_async_copy(source, dst, sem).wait()

    def conv(value, taps):
        taps = taps.astype(F32)
        row = lax.broadcasted_iota(jnp.int32, value.shape, 0)
        total = value * taps[2:3]
        total = total + jnp.where(row >= 1, pltpu.roll(value, 1, 0), 0.0) * taps[1:2]
        return total + jnp.where(row >= 2, pltpu.roll(value, 2, 0), 0.0) * taps[0:1]

    def sequence(s, carry):
        at = pl.ds(pl.multiple_of(s * span, span), span)
        a = mine[at, :].astype(F32)
        b = theirs[at, :].astype(F32)
        total = jnp.sum(a * a, axis=1, keepdims=True) + jnp.sum(b * b, axis=1, keepdims=True)
        inverse = lax.rsqrt(total / scale.shape[1] + norm_eps)
        low = jnp.where(core == 0, a, b)
        high = jnp.where(core == 0, b, a)
        half = a.shape[1]
        normed = jnp.concatenate(
            [
                (low * inverse * scale[:, 0:half].astype(F32)).astype(BF16),
                (high * inverse * scale[:, half:].astype(F32)).astype(BF16),
            ],
            axis=1,
        )
        value = dot(normed, w_up[:, 0:width]).astype(BF16).astype(F32)
        gate = dot(normed, w_up[:, width:]).astype(BF16).astype(F32)
        value = conv(value, taps_v[...])
        gate = conv(gate, taps_g[...])
        hidden[at, :] = (value * jax.nn.gelu(gate, approximate=True)).astype(BF16)
        return carry

    lax.fori_loop(0, 4, sequence, 0)


def contract_pair(pos, hidden, blocks, keep, send, weights, sems):
    y = pos[7]
    rows = weights.shape[2]
    width = weights.shape[3]
    waits = []
    for index, (where, choices) in enumerate(blocks):
        for j in range(2):
            dst = weights.at[where, y if j == 0 else 1 - y]
            sem = sems.at[index * 2 + j]
            copy_from(choices, sem, dst, lambda ref, b=j * rows: ref.at[pl.ds(b, rows), :])
            waits.append((choices[0][1].at[pl.ds(j * rows, rows), :], dst, sem))
    for source, dst, sem in waits:
        pltpu.make_async_copy(source, dst, sem).wait()
    for index, out in ((1, send), (0, keep)):
        for side in range(2):
            out[:, side * width : (side + 1) * width] = dot(
                hidden[...], weights[index, side]
            ).astype(BF16)


def contract_kernel_one(pos, hidden, slot_o, slot_r2, slot_l2, keep, send, weights, sems):
    z = pos[6]
    same = jnp.where((z // 2) == pos[5], 0, 1)
    low = z < 2
    blocks = (
        (same, ((None, slot_o),)),
        (1 - same, ((low, slot_l2), (jnp.logical_not(low), slot_r2))),
    )
    contract_pair(pos, hidden, blocks, keep, send, weights, sems)


def contract_kernel_two(
    pos, hidden, slot_r1, slot_l1, slot_r3, slot_l3, keep, send, weights, sems
):
    z, last = pos[6], pos[8]
    same = jnp.where((z // 2) == pos[5], 0, 1)
    even = lax.rem(z, 2) == 0
    blocks = (
        (same, ((even, slot_l1), (jnp.logical_not(even), slot_r1))),
        (
            1 - same,
            ((z == 0, slot_l3), (z == 1, slot_l1), (z == 2, slot_r1), (z == last, slot_r3)),
        ),
    )
    contract_pair(pos, hidden, blocks, keep, send, weights, sems)


def call(kernel, outs, args, scratch=(), flops=0, free=0):
    in_specs = [pl.BlockSpec(memory_space=pltpu.SMEM)]
    in_specs += [pl.BlockSpec(memory_space=pltpu.VMEM)] * (len(args) - 1 - free)
    in_specs += [pl.BlockSpec(memory_space=pl.ANY)] * free
    return pl.pallas_call(
        kernel,
        out_shape=[jax.ShapeDtypeStruct(*o) for o in outs],
        in_specs=in_specs,
        out_specs=[pl.BlockSpec(memory_space=pltpu.VMEM)] * len(outs),
        scratch_shapes=list(scratch),
        cost_estimate=pl.CostEstimate(flops=flops, bytes_accessed=1 << 20, transcendentals=0),
        compiler_params=pltpu.CompilerParams(vmem_limit_bytes=56 << 20),
    )(*args)


def plane_shards(sizes):
    n_x, n_z, n_y, n_c = sizes
    axes = ("rep", "z", "y", "tp")

    def pairs(move):
        found = []
        for x in range(n_x):
            for z in range(n_z):
                for y in range(n_y):
                    for c in range(n_c):
                        to = move(x, z, y, c)
                        if to is not None:
                            a = ((x * n_z + z) * n_y + y) * n_c + c
                            b = ((to[0] * n_z + to[1]) * n_y + to[2]) * n_c + to[3]
                            found.append((a, b))
        return found

    over_x = pairs(lambda x, z, y, c: (1 - x, z, y, c))
    over_y = pairs(lambda x, z, y, c: (x, z, 1 - y, c))
    over_d = pairs(lambda x, z, y, c: (1 - x, z, 1 - y, c))
    over_c = pairs(lambda x, z, y, c: (x, z, y, 1 - c))
    up_z = pairs(lambda x, z, y, c: (x, z + 1, y, c) if z + 1 < n_z else None)
    down_z = pairs(lambda x, z, y, c: (x, z - 1, y, c) if z > 0 else None)
    up_z2 = pairs(lambda x, z, y, c: (x, z + 1, y, c) if 1 <= z < n_z - 1 else None)
    down_z2 = pairs(lambda x, z, y, c: (x, z - 1, y, c) if 0 < z < n_z - 1 else None)
    up_z3 = pairs(lambda x, z, y, c: (x, z + 1, y, c) if z == n_z - 2 else None)
    down_z3 = pairs(lambda x, z, y, c: (x, z - 1, y, c) if z == 1 else None)

    def move(value, perm):
        return lax.ppermute(value, axes, perm)

    def gather(own, received):
        slot = jnp.concatenate([own, received], axis=0)
        r1 = move(slot, up_z)
        l1 = move(slot, down_z)
        r2 = move(r1, up_z2)
        l2 = move(l1, down_z2)
        r3 = move(r2, up_z3)
        l3 = move(l2, down_z3)
        return slot, r1, l1, r2, l2, r3, l3

    def shards(
        incoming_features,
        attend_prenormal_scale,
        probe_matrix,
        lookup_matrix,
        content_matrix,
        forgetting_matrix,
        result_switch_matrix,
        forgetting_shift,
        spike_forget_logarithm,
        attend_unit_scale,
        attend_result_matrix,
        perceptron_scale,
        content_expand_matrix,
        switch_expand_matrix,
        content_kernel,
        switch_kernel,
        contract_matrix,
    ):
        x, z, y, c = (lax.axis_index(axis) for axis in axes)
        quarter = 2 * x + y
        pos = jnp.stack(
            [
                quarter,
                2 * x + (1 - y),
                2 * (1 - x) + y,
                2 * x + (1 - y),
                2 * (1 - x) + (1 - y),
                c,
                z,
                y,
                jnp.int32(n_z - 1),
            ]
        ).astype(jnp.int32)
        span, width = incoming_features.shape
        embed = width * n_c
        chunk = probe_matrix.shape[0]
        part = attend_result_matrix.shape[0] // 4
        pack_rows = 3 * chunk + 2 * part + chunk // 2
        own, send = call(
            pack_kernel,
            [((pack_rows, LANES), BF16)] * 2,
            (
                pos,
                probe_matrix,
                lookup_matrix,
                content_matrix,
                forgetting_matrix,
                result_switch_matrix,
                attend_result_matrix,
            ),
        )
        spike_o, to_x, to_y, to_d = call(
            input_kernel,
            [((span, LANES), BF16)] + [((span, width + LANES), BF16)] * 3,
            (pos, spike_forget_logarithm, incoming_features),
        )
        attn = gather(own, move(send, over_y))
        from_x = move(to_x, over_x)
        from_y = move(to_y, over_y)
        from_d = move(to_d, over_d)

        ff = content_expand_matrix.shape[1] // 4

        def up_part(index):
            return jnp.concatenate(
                [
                    lax.dynamic_slice_in_dim(content_expand_matrix, index * ff, ff, 1),
                    lax.dynamic_slice_in_dim(switch_expand_matrix, index * ff, ff, 1),
                ],
                axis=1,
            )

        def down_part(index):
            return lax.dynamic_slice_in_dim(contract_matrix, index * ff, ff, 0)

        across = 2 * x + (1 - y)
        up = gather(up_part(quarter), move(up_part(across), over_y))
        down = gather(down_part(quarter), move(down_part(across), over_y))

        def halves(blocks):
            mine = jnp.concatenate(blocks, axis=0)
            return mine, move(mine, over_c)

        def reduce(keep, other):
            total = (keep.astype(F32) + other.astype(F32)).astype(BF16)
            blocks = [total[i * span : (i + 1) * span] for i in range(4)]
            return (
                blocks[0], move(blocks[1], over_x), move(blocks[2], over_y), move(blocks[3], over_d)
            )

        def add_up(base, parts):
            total = parts[0].astype(F32)
            for part_ in parts[1:]:
                total = total + part_.astype(F32)
            return (base.astype(F32) + total.astype(BF16).astype(F32)).astype(BF16)

        tokens = 4 * span
        mine, theirs = halves(
            [incoming_features] + [value[:, :width] for value in (from_x, from_y, from_d)],
        )
        key_w = forgetting_shift.shape[0] // 4
        val_w = attend_unit_scale.shape[0] // 4
        shift = lax.dynamic_slice_in_dim(forgetting_shift, quarter * key_w, key_w, 0)
        shift = jnp.concatenate([shift, shift]).reshape(1, LANES)
        unit = lax.dynamic_slice_in_dim(attend_unit_scale, quarter * val_w, val_w, 0)
        keep, other = call(
            attend_kernel,
            [((tokens, width), BF16)] * 2,
            (
                pos,
                mine,
                theirs,
                attend_prenormal_scale.reshape(1, embed),
                shift,
                unit.reshape(1, val_w),
                spike_o,
                from_x,
                from_y,
                from_d,
            )
            + attn,
            scratch=[
                pltpu.VMEM((embed, LANES), BF16),
                pltpu.VMEM((embed, 2 * LANES), BF16),
                pltpu.VMEM((embed, LANES), BF16),
                pltpu.VMEM((8, part, embed // 8), BF16),
                pltpu.VMEM((8, chunk // 2, LANES), BF16),
                pltpu.VMEM((tokens, LANES), F32),
                pltpu.VMEM((tokens, LANES), BF16),
                pltpu.VMEM((tokens, LANES), BF16),
                pltpu.VMEM((tokens, LANES), F32),
                pltpu.VMEM((tokens, LANES), BF16),
                pltpu.SemaphoreType.DMA((48,)),
            ],
            flops=10**10,
            free=7,
        )
        middle = add_up(incoming_features, reduce(keep, move(other, over_c)))
        mine, theirs = halves(
            [middle, move(middle, over_x), move(middle, over_y), move(middle, over_d)],
        )
        taps_v = lax.dynamic_slice_in_dim(content_kernel, quarter * ff, ff, 1)
        taps_g = lax.dynamic_slice_in_dim(switch_kernel, quarter * ff, ff, 1)
        (hidden,) = call(
            expand_kernel,
            [((tokens, ff), BF16)],
            (pos, mine, theirs, perceptron_scale.reshape(1, embed), taps_v, taps_g) + up,
            scratch=[pltpu.VMEM((embed, 2 * ff), BF16), pltpu.SemaphoreType.DMA((8,))],
            flops=10**10,
            free=7,
        )
        half = width // 2
        slot_o, slot_r1, slot_l1, slot_r2, slot_l2, slot_r3, slot_l3 = down
        parts = []
        for kernel, slots in (
            (contract_kernel_one, (slot_o, slot_r2, slot_l2)),
            (contract_kernel_two, (slot_r1, slot_l1, slot_r3, slot_l3)),
        ):
            keep, other = call(
                kernel,
                [((tokens, half), BF16)] * 2,
                (pos, hidden) + slots,
                scratch=[
                    pltpu.VMEM((2, 2, ff, embed // 8), BF16),
                    pltpu.SemaphoreType.DMA((4,)),
                ],
                flops=10**10,
                free=len(slots),
            )
            pieces = reduce(keep, move(other, over_c))
            total = pieces[0].astype(F32)
            for piece in pieces[1:]:
                total = total + piece.astype(F32)
            parts.append(total.astype(BF16).astype(F32))
        even = lax.rem(z, 2) == 0
        ffn = jnp.concatenate(
            [jnp.where(even, parts[0], parts[1]), jnp.where(even, parts[1], parts[0])], axis=1
        )
        return (middle.astype(F32) + ffn).astype(BF16)

    return shards


def plane_sizes(mesh):
    if tuple(mesh.axis_names) != ("rep", "fs", "tp"):
        return None
    n_x, n_fs, n_c = (mesh.shape[axis] for axis in ("rep", "fs", "tp"))
    if n_x != 2 or n_c != 2 or n_fs % 2 or n_fs // 2 != 4:
        return None
    return (n_x, n_fs // 2, 2, n_c)


def solution(mesh):
    sizes = plane_sizes(mesh)
    if sizes is None:
        body, seq = general_shards, ("rep", "fs")
        weight = ("fs",)
        used = mesh
    else:
        body, seq = plane_shards(sizes), ("rep", "z", "y")
        weight = ("z", "y")
        used = Mesh(mesh.devices.reshape(sizes), ("rep", "z", "y", "tp"))
    placed = (
        P(seq, "tp"),
        P(),
        P(weight, "tp"),
        P(weight, "tp"),
        P(weight, "tp"),
        P(weight, "tp"),
        P(weight, "tp"),
        P("tp"),
        P(seq, "tp"),
        P("tp"),
        P("tp", weight),
        P(),
        P(weight, "tp"),
        P(weight, "tp"),
        P(None, "tp"),
        P(None, "tp"),
        P("tp", weight),
    )
    return jax.shard_map(body, mesh=used, in_specs=placed, out_specs=P(seq, "tp"), check_vma=False)
```

```python
import jax
import jax.numpy as jnp
from jax import lax
from jax.experimental import pallas as pl
from jax.experimental.pallas import tpu as pltpu
from jax.sharding import Mesh
from jax.sharding import PartitionSpec as P


HEAD_K = 32
HEAD_V = 64
BLOCK = 64
SUB = 8
LANES = 128

norm_eps = 1e-06
switch_multiplier = 16.0


def row_norm(content_tokens, gain):
    content_tokens = content_tokens.astype(jnp.float32)
    scaled = content_tokens * lax.rsqrt(
        jnp.mean(content_tokens * content_tokens, axis=-1, keepdims=True) + norm_eps
    )
    return (scaled * gain.astype(jnp.float32)).astype(jnp.bfloat16)


def gated_scan(probe_tokens, lookup_tokens, content_tokens, forgetting_scores):
    length, heads, key_size = probe_tokens.shape
    value_size = content_tokens.shape[-1]
    blocks = length // BLOCK

    def split_blocks(array):
        return array.reshape(blocks, BLOCK, heads, array.shape[-1])

    causal = jnp.arange(BLOCK)[:, None] >= jnp.arange(BLOCK)[None, :]
    highest = lax.Precision.HIGHEST

    def step(state, incoming_tokens):
        query_block, key_block, value_block, decay_block = incoming_tokens
        cumulative = jnp.cumsum(decay_block, axis=0)
        differ = cumulative[:, None] - cumulative[None, :]
        weight = jnp.exp(jnp.where(causal[:, :, None, None], differ, -jnp.inf))
        scores = jnp.einsum("thd,shd,tshd->tsh", query_block, key_block, weight, precision=highest)
        inner = jnp.einsum("tsh,shv->thv", scores, value_block, precision=highest)
        carried = jnp.einsum(
            "thd,hdv->thv", query_block * jnp.exp(cumulative), state, precision=highest
        )
        final = cumulative[-1]
        state = jnp.exp(final)[:, :, None] * state + jnp.einsum(
            "shd,shv->hdv",
            key_block * jnp.exp(final[None] - cumulative),
            value_block,
            precision=highest,
        )
        return (state, inner + carried)

    start_state = jnp.zeros((heads, key_size, value_size), jnp.float32)
    _, result_tokens = lax.scan(
        step,
        start_state,
        (
            split_blocks(probe_tokens),
            split_blocks(lookup_tokens),
            split_blocks(content_tokens),
            split_blocks(forgetting_scores),
        ),
    )
    return result_tokens.reshape(length, heads, value_size)


def attend_unit_results(
    probe_tokens,
    lookup_tokens,
    content_tokens,
    result_switch,
    forgetting_raw,
    spike_forgetting,
    attend_unit_scale,
):
    length = probe_tokens.shape[0]
    heads = probe_tokens.shape[1] // HEAD_K
    forgetting_scores = jax.nn.log_sigmoid(forgetting_raw) / switch_multiplier + spike_forgetting

    def split_heads(array, width):
        return array.astype(jnp.float32).reshape(length, heads, width)

    result_tokens = gated_scan(
        split_heads(probe_tokens, HEAD_K) * HEAD_K ** (-0.5),
        split_heads(lookup_tokens, HEAD_K),
        split_heads(content_tokens, HEAD_V),
        split_heads(forgetting_scores, HEAD_K),
    )
    result_tokens = result_tokens * lax.rsqrt(
        jnp.mean(result_tokens * result_tokens, axis=-1, keepdims=True) + norm_eps
    )
    result_tokens = result_tokens * attend_unit_scale.astype(jnp.float32).reshape(heads, HEAD_V)
    switched_result = result_tokens.reshape(length, heads * HEAD_V) * jax.nn.silu(
        result_switch.astype(jnp.float32)
    )
    return switched_result.astype(jnp.bfloat16)


def causal_conv(content_tokens, taps):
    content_tokens = content_tokens.astype(jnp.float32)
    taps = taps.astype(jnp.float32)
    width = taps.shape[0]
    padded = jnp.pad(content_tokens, ((width - 1, 0), (0, 0)))
    total = jnp.zeros_like(content_tokens)
    for offset in range(width):
        total = total + padded[offset : offset + content_tokens.shape[0]] * taps[offset]
    return total


def general_shards(
    incoming_features,
    attend_prenormal_scale,
    probe_matrix,
    lookup_matrix,
    content_matrix,
    forgetting_matrix,
    result_switch_matrix,
    forgetting_shift,
    spike_forget_logarithm,
    attend_unit_scale,
    attend_result_matrix,
    perceptron_scale,
    content_expand_matrix,
    switch_expand_matrix,
    content_kernel,
    switch_kernel,
    contract_matrix,
):
    whole_in = lax.all_gather(incoming_features, "tp", axis=1, tiled=True)
    columns = row_norm(whole_in, attend_prenormal_scale)
    pieces = tuple(
        lax.all_gather(piece, "fs", axis=0, tiled=True)
        for piece in (
            probe_matrix,
            lookup_matrix,
            content_matrix,
            forgetting_matrix,
            result_switch_matrix,
        )
    )
    query_sum, key_sum, value_sum, decay_sum, gate_sum = tuple(
        (jnp.dot(columns, piece, preferred_element_type=jnp.float32) for piece in pieces)
    )
    switched_result = attend_unit_results(
        query_sum.astype(jnp.bfloat16),
        key_sum.astype(jnp.bfloat16),
        value_sum.astype(jnp.bfloat16),
        gate_sum.astype(jnp.bfloat16),
        decay_sum + forgetting_shift,
        spike_forget_logarithm,
        attend_unit_scale,
    )
    mixer_partial = jnp.dot(
        switched_result,
        lax.all_gather(attend_result_matrix, "fs", axis=1, tiled=True),
        preferred_element_type=jnp.float32,
    )
    mix = lax.psum_scatter(
        mixer_partial.astype(jnp.bfloat16), "tp", scatter_dimension=1, tiled=True
    )
    middle = (
        incoming_features.astype(jnp.float32) + lax.optimization_barrier(mix).astype(jnp.float32)
    ).astype(jnp.bfloat16)
    whole_mid = lax.all_gather(middle, "tp", axis=1, tiled=True)
    columns = row_norm(whole_mid, perceptron_scale)
    pieces = (
        lax.all_gather(content_expand_matrix, "fs", axis=0, tiled=True),
        lax.all_gather(switch_expand_matrix, "fs", axis=0, tiled=True),
    )
    value_total = jnp.dot(columns, pieces[0], preferred_element_type=jnp.float32)
    gate_total = jnp.dot(columns, pieces[1], preferred_element_type=jnp.float32)
    conv_value = causal_conv(value_total.astype(jnp.bfloat16), content_kernel)
    conv_gated = causal_conv(gate_total.astype(jnp.bfloat16), switch_kernel)
    hidden = (conv_value * jax.nn.gelu(conv_gated, approximate=True)).astype(jnp.bfloat16)
    down_partial = jnp.dot(
        hidden,
        lax.all_gather(contract_matrix, "fs", axis=1, tiled=True),
        preferred_element_type=jnp.float32,
    )
    ffn = lax.psum_scatter(down_partial.astype(jnp.bfloat16), "tp", scatter_dimension=1, tiled=True)
    return (middle.astype(jnp.float32) + lax.optimization_barrier(ffn).astype(jnp.float32)).astype(
        jnp.bfloat16
    )


F32 = jnp.float32
BF16 = jnp.bfloat16


def dot(a, b):
    return jnp.dot(a, b, preferred_element_type=F32)


def pack_kernel(pos, probe, lookup, content, forget, switch, result, own, send):
    quarter, across = pos[0], pos[1]
    rows = probe.shape[0]
    half = rows // 2
    key_w = probe.shape[1] // 4
    val_w = content.shape[1] // 4
    part = result.shape[0] // 4

    def pack(index, out):
        for q in range(4):

            @pl.when(index == q)
            def _():
                keys = pl.ds(q * key_w, key_w)
                vals = pl.ds(q * val_w, val_w)
                out[0:rows, :] = jnp.concatenate([probe[:, keys], lookup[:, keys]], axis=1)
                out[rows : 2 * rows, :] = content[:, vals]
                out[2 * rows : 3 * rows, :] = switch[:, vals]
                base = 3 * rows
                out[base : base + part, :] = result[q * part : (q + 1) * part, 0:LANES]
                out[base + part : base + 2 * part, :] = result[q * part : (q + 1) * part, LANES:]
                base = base + 2 * part
                decay = forget[:, keys]
                out[base : base + half, :] = jnp.concatenate(
                    [decay[:half], decay[half:]], axis=1
                )

    pack(across, send)
    pack(quarter, own)


def input_kernel(pos, spike, feat, own_spike, to_x, to_y, to_d):
    key_w = spike.shape[1] // 4
    width = feat.shape[1]

    def spikes(index):
        value = spike[:, 0:key_w]
        for q in range(1, 4):
            value = jnp.where(index == q, spike[:, q * key_w : (q + 1) * key_w], value)
        high = value.astype(BF16)
        low = (value - high.astype(F32)).astype(BF16)
        return jnp.concatenate([high, low], axis=1)

    own_spike[...] = spikes(pos[0])
    for slot, ref in ((2, to_x), (3, to_y), (4, to_d)):
        ref[:, 0:width] = feat[...]
        ref[:, width:] = spikes(pos[slot])


def copy_from(choices, sem, dst, cut):
    for cond, ref in choices:
        copy = pltpu.make_async_copy(cut(ref), dst, sem)
        if cond is None:
            copy.start()
        else:
            pl.when(cond)(copy.start)


def blocks_of(pos, slots):
    slot_o, slot_r1, slot_l1, slot_r2, slot_l2, slot_r3, slot_l3 = slots
    z, last = pos[6], pos[8]
    low = z < 2
    first_z = z == 0
    last_z = z == last
    return (
        (z, ((None, slot_o),)),
        (jnp.bitwise_xor(z, 2), ((low, slot_l2), (jnp.logical_not(low), slot_r2))),
        (
            jnp.where(first_z, last, z - 1),
            ((first_z, slot_l3), (jnp.logical_not(first_z), slot_r1)),
        ),
        (
            jnp.where(last_z, 0, z + 1),
            ((last_z, slot_r3), (jnp.logical_not(last_z), slot_l1)),
        ),
    )


def attend_kernel(
    pos, mine, theirs, scale, shift, unit, spike_o, spike_x, spike_y, spike_d,
    slot_o, slot_r1, slot_l1, slot_r2, slot_l2, slot_r3, slot_l3,
    keep, send,
    w_qk, w_vg, w_f, w_o, folded, qk_s, v_s, g_s, f_s, gated, sems,
):
    core, y = pos[5], pos[7]
    rows = slot_o.shape[0] // 2
    chunk = w_qk.shape[0] // 8
    half = chunk // 2
    part = w_o.shape[1]
    span = spike_o.shape[0]
    length, width = mine.shape
    key_w = f_s.shape[1] // 2

    slots = (slot_o, slot_r1, slot_l1, slot_r2, slot_l2, slot_r3, slot_l3)
    waits = []
    for index, (zi, choices) in enumerate(blocks_of(pos, slots)):
        for j in range(2):
            shard = zi * 2 + (y if j == 0 else 1 - y)
            at = pl.ds(pl.multiple_of(shard * chunk, chunk), chunk)
            base = j * rows
            targets = (
                (w_qk.at[at, :], chunk),
                (w_vg.at[at, 0:LANES], chunk),
                (w_vg.at[at, LANES : 2 * LANES], chunk),
                (w_o.at[shard, :, 0:LANES], part),
                (w_o.at[shard, :, LANES : 2 * LANES], part),
                (folded.at[shard], half),
            )
            for k, (dst, size) in enumerate(targets):
                sem = sems.at[index * 12 + j * 6 + k]
                copy_from(choices, sem, dst, lambda ref, b=base, n=size: ref.at[pl.ds(b, n), :])
                waits.append((slot_o.at[pl.ds(base, size), :], dst, sem))
                base += size
    for source, dst, sem in waits:
        pltpu.make_async_copy(source, dst, sem).wait()
    for shard in range(8):
        w_f[shard * chunk : shard * chunk + half, :] = folded[shard]
        w_f[shard * chunk + half : (shard + 1) * chunk, :] = pltpu.roll(
            folded[shard].astype(F32), key_w, 1
        ).astype(BF16)

    def project(s, carry):
        at = pl.ds(pl.multiple_of(s * span, span), span)
        a = mine[at, :].astype(F32)
        b = theirs[at, :].astype(F32)
        total = jnp.sum(a * a, axis=1, keepdims=True) + jnp.sum(b * b, axis=1, keepdims=True)
        inverse = lax.rsqrt(total / scale.shape[1] + norm_eps)
        low = jnp.where(core == 0, a, b)
        high = jnp.where(core == 0, b, a)
        width = a.shape[1]
        normed = jnp.concatenate(
            [
                (low * inverse * scale[:, 0:width].astype(F32)).astype(BF16),
                (high * inverse * scale[:, width:].astype(F32)).astype(BF16),
            ],
            axis=1,
        )
        qk_s[at, :] = dot(normed, w_qk[...]).astype(BF16).astype(F32)
        vg = dot(normed, w_vg[...]).astype(BF16)
        v_s[at, :] = vg[:, 0:LANES]
        g_s[at, :] = vg[:, LANES:]
        f_s[at, :] = dot(normed, w_f[...])
        return carry

    count = length // span
    lax.fori_loop(0, count, project, 0)

    lane = lax.broadcasted_iota(jnp.int32, (span, LANES), 1)
    left = lane < key_w
    row = lax.broadcasted_iota(jnp.int32, (span, LANES), 0)
    lane_head = lax.broadcasted_iota(jnp.int32, (LANES, 2 * LANES), 0) // HEAD_K
    wide_head = lax.broadcasted_iota(jnp.int32, (LANES, 2 * LANES), 1) // HEAD_V
    spread = (lane_head == wide_head).astype(BF16)
    wide_a = lax.broadcasted_iota(jnp.int32, (2 * LANES, 2 * LANES), 0) // HEAD_V
    wide_b = lax.broadcasted_iota(jnp.int32, (2 * LANES, 2 * LANES), 1) // HEAD_V
    same_wide = (wide_a == wide_b).astype(BF16)
    tri = (
        lax.broadcasted_iota(jnp.int32, (span, span), 0)
        >= lax.broadcasted_iota(jnp.int32, (span, span), 1)
    ).astype(BF16)
    heads = LANES // HEAD_K

    def split_dot(a, value):
        one = value.astype(BF16)
        rest = value - one.astype(F32)
        two = rest.astype(BF16)
        three = (rest - two.astype(F32)).astype(BF16)
        return dot(a, one) + dot(a, two) + dot(a, three)

    def pair(p, carry):
        at_a = pl.ds(pl.multiple_of(p * 2 * span, span), span)
        at_b = pl.ds(pl.multiple_of(p * 2 * span + span, span), span)
        qk_a, qk_b = qk_s[at_a, :], qk_s[at_b, :]
        query = jnp.where(left, qk_a, pltpu.roll(qk_b, key_w, 1)) * HEAD_K ** (-0.5)
        keys = jnp.where(left, pltpu.roll(qk_a, key_w, 1), qk_b)
        v_a, v_b = v_s[at_a, :], v_s[at_b, :]
        value = jnp.concatenate([v_a, v_b], axis=1)
        decay = jnp.where(left, f_s[at_a, :], pltpu.roll(f_s[at_b, :], key_w, 1))
        decay = decay + shift[...]
        spike_a = jnp.where(p == 0, spike_o[...], spike_y[:, width:]).astype(F32)
        spike_b = jnp.where(p == 0, spike_x[:, width:], spike_d[:, width:]).astype(F32)
        spike_a = spike_a + pltpu.roll(spike_a, key_w, 1)
        spike_b = spike_b + pltpu.roll(spike_b, key_w, 1)
        soft = jnp.minimum(decay, 0.0) - jnp.log1p(jnp.exp(-jnp.abs(decay)))
        log_decay = soft / switch_multiplier + jnp.where(left, spike_a, spike_b)
        cum = split_dot(tri, log_decay)

        tiles = span // SUB
        q3 = query.reshape(tiles, SUB, LANES)
        k3 = keys.reshape(tiles, SUB, LANES)
        c3 = cum.reshape(tiles, SUB, LANES)
        valuef = value.astype(F32)
        v3 = valuef.reshape(tiles, SUB, 2 * LANES)
        place = lax.broadcasted_iota(jnp.int32, (tiles, SUB, LANES), 1)
        out = jnp.zeros((span, 2 * LANES), F32)
        for lag in range(SUB):
            if lag == 0:
                term = q3 * k3
                v_lag = v3
            else:
                k_lag = pltpu.roll(k3, lag, 1)
                c_lag = pltpu.roll(c3, lag, 1)
                v_lag = pltpu.roll(v3, lag, 1)
                fall = jnp.exp(jnp.where(place >= lag, c3 - c_lag, -jnp.inf))
                term = q3 * k_lag * fall
            spread_term = dot(term.reshape(span, LANES).astype(BF16), spread)
            out = out + spread_term * v_lag.reshape(span, 2 * LANES)

        size = SUB
        while size < span:
            blocks = max(span // (2 * size), 1)
            if 2 * size > span:
                second_rows = span - size
            else:
                second_rows = size
            begin = [i * 2 * size for i in range(blocks)]
            q_parts, k_parts, v_parts = [], [], []
            for b0 in begin:
                middle = b0 + size
                ref_row = cum[middle - 1 : middle, :]
                q_parts.append(
                    query[middle : middle + second_rows]
                    * jnp.exp(cum[middle : middle + second_rows] - ref_row)
                )
                k_parts.append(keys[b0:middle] * jnp.exp(ref_row - cum[b0:middle]))
                v_parts.append(value[b0:middle] if size % 16 == 0 else valuef[b0:middle])
            q_all = jnp.concatenate(q_parts, axis=0) if blocks > 1 else q_parts[0]
            k_all = jnp.concatenate(k_parts, axis=0) if blocks > 1 else k_parts[0]
            v_all = (jnp.concatenate(v_parts, axis=0) if blocks > 1 else v_parts[0]).astype(BF16)
            n_q, n_k = q_all.shape[0], k_all.shape[0]
            q_lane = lax.broadcasted_iota(jnp.int32, (n_q, LANES), 1) // HEAD_K
            q_heads = jnp.concatenate(
                [jnp.where(q_lane == h, q_all, 0.0) for h in range(heads)], axis=0
            ).astype(BF16)
            scores = lax.dot_general(
                q_heads, k_all.astype(BF16), (((1,), (1,)), ((), ())), preferred_element_type=F32
            )
            if blocks > 1:
                q_block = (
                    lax.rem(lax.broadcasted_iota(jnp.int32, (heads * n_q, n_k), 0), n_q)
                    // second_rows
                )
                k_block = lax.broadcasted_iota(jnp.int32, (heads * n_q, n_k), 1) // size
                scores = jnp.where(q_block == k_block, scores, 0.0)
            wide = dot(scores.astype(BF16), v_all)
            wide_lane = lax.broadcasted_iota(jnp.int32, (n_q, 2 * LANES), 1) // HEAD_V
            total = wide[0:n_q]
            for h in range(1, heads):
                total = jnp.where(wide_lane == h, wide[h * n_q : (h + 1) * n_q], total)
            zeros = jnp.zeros((size, 2 * LANES), F32)
            full = []
            for i in range(blocks):
                full.append(zeros)
                full.append(total[i * second_rows : (i + 1) * second_rows])
            covered = blocks * size + blocks * second_rows
            if covered < span:
                full.append(jnp.zeros((span - covered, 2 * LANES), F32))
            out = out + jnp.concatenate(full, axis=0)
            size *= 2

        square = out * out
        high = square.astype(BF16)
        low = (square - high.astype(F32)).astype(BF16)
        mean = (dot(high, same_wide) + dot(low, same_wide)) / HEAD_V
        out = out * lax.rsqrt(mean + norm_eps)
        gate = jnp.concatenate([g_s[at_a, :], g_s[at_b, :]], axis=1).astype(F32)
        gain = unit[...].astype(F32)
        out = out * jnp.concatenate([gain, gain], axis=1)
        out = out * (gate / (1.0 + jnp.exp(-gate)))
        gated[at_a, :] = out[:, 0:LANES].astype(BF16)
        gated[at_b, :] = out[:, LANES:].astype(BF16)
        return carry

    lax.fori_loop(0, count // 2, pair, 0)
    mix_out(core, gated, w_o, keep, send)


def mix_out(core, left, weights, keep, send):
    shards = weights.shape[0]
    width = weights.shape[2]
    for h in range(2):
        for f in range(shards // 2):
            w = weights[h * (shards // 2) + f]
            value = dot(left[...], w).astype(BF16)
            cols = slice(f * width, (f + 1) * width)

            @pl.when(core == h)
            def _():
                keep[:, cols] = value

            @pl.when(core != h)
            def _():
                send[:, cols] = value


def expand_kernel(
    pos, mine, theirs, scale, taps_v, taps_g,
    *refs,
):
    own, received = refs[0:7], refs[7:14]
    hidden, w_up, sems = refs[14:]
    core, y = pos[5], pos[7]
    chunk = own[0].shape[0]
    span = hidden.shape[0] // 4
    width = hidden.shape[1]

    waits = []
    for j, slots in enumerate((own, received)):
        side = y if j == 0 else 1 - y
        for index, (zi, choices) in enumerate(blocks_of(pos, slots)):
            dst = w_up.at[pl.ds(pl.multiple_of((zi * 2 + side) * chunk, chunk), chunk), :]
            sem = sems.at[index * 2 + j]
            copy_from(choices, sem, dst, lambda ref: ref)
            waits.append((slots[0], dst, sem))
    for source, dst, sem in waits:
        pltpu.make_async_copy(source, dst, sem).wait()

    def conv(value, taps):
        taps = taps.astype(F32)
        row = lax.broadcasted_iota(jnp.int32, value.shape, 0)
        total = value * taps[2:3]
        total = total + jnp.where(row >= 1, pltpu.roll(value, 1, 0), 0.0) * taps[1:2]
        return total + jnp.where(row >= 2, pltpu.roll(value, 2, 0), 0.0) * taps[0:1]

    def sequence(s, carry):
        at = pl.ds(pl.multiple_of(s * span, span), span)
        a = mine[at, :].astype(F32)
        b = theirs[at, :].astype(F32)
        total = jnp.sum(a * a, axis=1, keepdims=True) + jnp.sum(b * b, axis=1, keepdims=True)
        inverse = lax.rsqrt(total / scale.shape[1] + norm_eps)
        low = jnp.where(core == 0, a, b)
        high = jnp.where(core == 0, b, a)
        half = a.shape[1]
        normed = jnp.concatenate(
            [
                (low * inverse * scale[:, 0:half].astype(F32)).astype(BF16),
                (high * inverse * scale[:, half:].astype(F32)).astype(BF16),
            ],
            axis=1,
        )
        value = dot(normed, w_up[:, 0:width]).astype(BF16).astype(F32)
        gate = dot(normed, w_up[:, width:]).astype(BF16).astype(F32)
        value = conv(value, taps_v[...])
        gate = conv(gate, taps_g[...])
        hidden[at, :] = (value * jax.nn.gelu(gate, approximate=True)).astype(BF16)
        return carry

    lax.fori_loop(0, 4, sequence, 0)


def contract_pair(pos, hidden, shards, keep, send, weights, sems):
    y = pos[7]
    width = weights.shape[3]
    waits = []
    for j, blocks in enumerate(shards):
        for index, (where, choices) in enumerate(blocks):
            dst = weights.at[where, y if j == 0 else 1 - y]
            sem = sems.at[index * 2 + j]
            copy_from(choices, sem, dst, lambda ref: ref)
            waits.append((choices[0][1], dst, sem))
    for source, dst, sem in waits:
        pltpu.make_async_copy(source, dst, sem).wait()
    for index, out in ((1, send), (0, keep)):
        for side in range(2):
            out[:, side * width : (side + 1) * width] = dot(
                hidden[...], weights[index, side]
            ).astype(BF16)


def contract_kernel_one(pos, hidden, *refs):
    z = pos[6]
    same = jnp.where((z // 2) == pos[5], 0, 1)
    low = z < 2

    def blocks(slot_o, slot_r2, slot_l2):
        return (
            (same, ((None, slot_o),)),
            (1 - same, ((low, slot_l2), (jnp.logical_not(low), slot_r2))),
        )

    contract_pair(pos, hidden, (blocks(*refs[0:3]), blocks(*refs[3:6])), *refs[6:])


def contract_kernel_two(pos, hidden, *refs):
    z, last = pos[6], pos[8]
    same = jnp.where((z // 2) == pos[5], 0, 1)
    even = lax.rem(z, 2) == 0

    def blocks(slot_r1, slot_l1, slot_r3, slot_l3):
        return (
            (same, ((even, slot_l1), (jnp.logical_not(even), slot_r1))),
            (
                1 - same,
                ((z == 0, slot_l3), (z == 1, slot_l1), (z == 2, slot_r1), (z == last, slot_r3)),
            ),
        )

    contract_pair(pos, hidden, (blocks(*refs[0:4]), blocks(*refs[4:8])), *refs[8:])


def call(kernel, outs, args, scratch=(), flops=0, free=0, grant=24):
    in_specs = [pl.BlockSpec(memory_space=pltpu.SMEM)]
    in_specs += [pl.BlockSpec(memory_space=pltpu.VMEM)] * (len(args) - 1 - free)
    in_specs += [pl.BlockSpec(memory_space=pl.ANY)] * free
    return pl.pallas_call(
        kernel,
        out_shape=[jax.ShapeDtypeStruct(*o) for o in outs],
        in_specs=in_specs,
        out_specs=[pl.BlockSpec(memory_space=pltpu.VMEM)] * len(outs),
        scratch_shapes=list(scratch),
        cost_estimate=pl.CostEstimate(flops=flops, bytes_accessed=1 << 20, transcendentals=0),
        compiler_params=pltpu.CompilerParams(vmem_limit_bytes=grant << 20),
    )(*args)


def plane_shards(sizes):
    n_x, n_z, n_y, n_c = sizes
    axes = ("rep", "z", "y", "tp")

    def pairs(move):
        found = []
        for x in range(n_x):
            for z in range(n_z):
                for y in range(n_y):
                    for c in range(n_c):
                        to = move(x, z, y, c)
                        if to is not None:
                            a = ((x * n_z + z) * n_y + y) * n_c + c
                            b = ((to[0] * n_z + to[1]) * n_y + to[2]) * n_c + to[3]
                            found.append((a, b))
        return found

    over_x = pairs(lambda x, z, y, c: (1 - x, z, y, c))
    over_y = pairs(lambda x, z, y, c: (x, z, 1 - y, c))
    over_d = pairs(lambda x, z, y, c: (1 - x, z, 1 - y, c))
    over_c = pairs(lambda x, z, y, c: (x, z, y, 1 - c))
    up_z = pairs(lambda x, z, y, c: (x, z + 1, y, c) if z + 1 < n_z else None)
    down_z = pairs(lambda x, z, y, c: (x, z - 1, y, c) if z > 0 else None)
    up_z2 = pairs(lambda x, z, y, c: (x, z + 1, y, c) if 1 <= z < n_z - 1 else None)
    down_z2 = pairs(lambda x, z, y, c: (x, z - 1, y, c) if 0 < z < n_z - 1 else None)
    up_z3 = pairs(lambda x, z, y, c: (x, z + 1, y, c) if z == n_z - 2 else None)
    down_z3 = pairs(lambda x, z, y, c: (x, z - 1, y, c) if z == 1 else None)

    up_z3_direct = pairs(lambda x, z, y, c: (x, n_z - 1, y, c) if z == n_z - 3 else None)
    down_z3_direct = pairs(lambda x, z, y, c: (x, 0, y, c) if z == 2 else None)

    def move(value, perm):
        return lax.ppermute(value, axes, perm)

    def gather(slot, direct=False):
        r1 = move(slot, up_z)
        l1 = move(slot, down_z)
        r2 = move(r1, up_z2)
        l2 = move(l1, down_z2)
        if direct:
            r3 = move(r1, up_z3_direct)
            l3 = move(l1, down_z3_direct)
        else:
            r3 = move(r2, up_z3)
            l3 = move(l2, down_z3)
        return slot, r1, l1, r2, l2, r3, l3

    def shards(
        incoming_features,
        attend_prenormal_scale,
        probe_matrix,
        lookup_matrix,
        content_matrix,
        forgetting_matrix,
        result_switch_matrix,
        forgetting_shift,
        spike_forget_logarithm,
        attend_unit_scale,
        attend_result_matrix,
        perceptron_scale,
        content_expand_matrix,
        switch_expand_matrix,
        content_kernel,
        switch_kernel,
        contract_matrix,
    ):
        x, z, y, c = (lax.axis_index(axis) for axis in axes)
        quarter = 2 * x + y
        pos = jnp.stack(
            [
                quarter,
                2 * x + (1 - y),
                2 * (1 - x) + y,
                2 * x + (1 - y),
                2 * (1 - x) + (1 - y),
                c,
                z,
                y,
                jnp.int32(n_z - 1),
            ]
        ).astype(jnp.int32)
        span, width = incoming_features.shape
        embed = width * n_c
        chunk = probe_matrix.shape[0]
        part = attend_result_matrix.shape[0] // 4
        pack_rows = 3 * chunk + 2 * part + chunk // 2
        own, send = call(
            pack_kernel,
            [((pack_rows, LANES), BF16)] * 2,
            (
                pos,
                probe_matrix,
                lookup_matrix,
                content_matrix,
                forgetting_matrix,
                result_switch_matrix,
                attend_result_matrix,
            ),
            grant=56,
        )
        spike_o, to_x, to_y, to_d = call(
            input_kernel,
            [((span, LANES), BF16)] + [((span, width + LANES), BF16)] * 3,
            (pos, spike_forget_logarithm, incoming_features),
            grant=56,
        )
        attn = gather(jnp.concatenate([own, move(send, over_y)], axis=0))
        from_x = move(to_x, over_x)
        from_y = move(to_y, over_y)
        from_d = move(to_d, over_d)

        ff = content_expand_matrix.shape[1] // 4

        def up_part(index):
            return jnp.concatenate(
                [
                    lax.dynamic_slice_in_dim(content_expand_matrix, index * ff, ff, 1),
                    lax.dynamic_slice_in_dim(switch_expand_matrix, index * ff, ff, 1),
                ],
                axis=1,
            )

        def down_part(index):
            return lax.dynamic_slice_in_dim(contract_matrix, index * ff, ff, 0)

        across = 2 * x + (1 - y)
        up = gather(up_part(quarter))
        up = up + gather(move(up_part(across), over_y))
        down_own = gather(down_part(quarter), direct=True)
        down_across = gather(move(down_part(across), over_y))

        def halves(blocks):
            mine = jnp.concatenate(blocks, axis=0)
            return mine, move(mine, over_c)

        def reduce(keep, other):
            total = (keep.astype(F32) + other.astype(F32)).astype(BF16)
            blocks = [total[i * span : (i + 1) * span] for i in range(4)]
            return (
                blocks[0], move(blocks[1], over_x), move(blocks[2], over_y), move(blocks[3], over_d)
            )

        def add_up(base, parts):
            total = parts[0].astype(F32)
            for part_ in parts[1:]:
                total = total + part_.astype(F32)
            return (base.astype(F32) + total.astype(BF16).astype(F32)).astype(BF16)

        tokens = 4 * span
        mine, theirs = halves(
            [incoming_features] + [value[:, :width] for value in (from_x, from_y, from_d)],
        )
        key_w = forgetting_shift.shape[0] // 4
        val_w = attend_unit_scale.shape[0] // 4
        shift = lax.dynamic_slice_in_dim(forgetting_shift, quarter * key_w, key_w, 0)
        shift = jnp.concatenate([shift, shift]).reshape(1, LANES)
        unit = lax.dynamic_slice_in_dim(attend_unit_scale, quarter * val_w, val_w, 0)
        keep, other = call(
            attend_kernel,
            [((tokens, width), BF16)] * 2,
            (
                pos,
                mine,
                theirs,
                attend_prenormal_scale.reshape(1, embed),
                shift,
                unit.reshape(1, val_w),
                spike_o,
                from_x,
                from_y,
                from_d,
            )
            + attn,
            scratch=[
                pltpu.VMEM((embed, LANES), BF16),
                pltpu.VMEM((embed, 2 * LANES), BF16),
                pltpu.VMEM((embed, LANES), BF16),
                pltpu.VMEM((8, part, embed // 8), BF16),
                pltpu.VMEM((8, chunk // 2, LANES), BF16),
                pltpu.VMEM((tokens, LANES), F32),
                pltpu.VMEM((tokens, LANES), BF16),
                pltpu.VMEM((tokens, LANES), BF16),
                pltpu.VMEM((tokens, LANES), F32),
                pltpu.VMEM((tokens, LANES), BF16),
                pltpu.SemaphoreType.DMA((48,)),
            ],
            grant=56,
            flops=10**10,
            free=7,
        )
        middle = add_up(incoming_features, reduce(keep, move(other, over_c)))
        mine, theirs = halves(
            [middle, move(middle, over_x), move(middle, over_y), move(middle, over_d)],
        )
        taps_v = lax.dynamic_slice_in_dim(content_kernel, quarter * ff, ff, 1)
        taps_g = lax.dynamic_slice_in_dim(switch_kernel, quarter * ff, ff, 1)
        (hidden,) = call(
            expand_kernel,
            [((tokens, ff), BF16)],
            (pos, mine, theirs, perceptron_scale.reshape(1, embed), taps_v, taps_g) + up,
            scratch=[pltpu.VMEM((embed, 2 * ff), BF16), pltpu.SemaphoreType.DMA((8,))],
            flops=10**10,
            free=14,
        )
        half = width // 2
        parts = []
        for kernel, places in (
            (contract_kernel_one, (0, 3, 4)), (contract_kernel_two, (1, 2, 5, 6))
        ):
            slots = tuple(group[place] for group in (down_own, down_across) for place in places)
            keep, other = call(
                kernel,
                [((tokens, half), BF16)] * 2,
                (pos, hidden) + slots,
                scratch=[
                    pltpu.VMEM((2, 2, ff, embed // 8), BF16),
                    pltpu.SemaphoreType.DMA((4,)),
                ],
                flops=10**10,
                free=len(slots),
            )
            pieces = reduce(keep, move(other, over_c))
            total = pieces[0].astype(F32)
            for piece in pieces[1:]:
                total = total + piece.astype(F32)
            parts.append(total.astype(BF16).astype(F32))
        even = lax.rem(z, 2) == 0
        ffn = jnp.concatenate(
            [jnp.where(even, parts[0], parts[1]), jnp.where(even, parts[1], parts[0])], axis=1
        )
        return (middle.astype(F32) + ffn).astype(BF16)

    return shards


def plane_sizes(mesh):
    if tuple(mesh.axis_names) != ("rep", "fs", "tp"):
        return None
    n_x, n_fs, n_c = (mesh.shape[axis] for axis in ("rep", "fs", "tp"))
    if n_x != 2 or n_c != 2 or n_fs % 2 or n_fs // 2 != 4:
        return None
    return (n_x, n_fs // 2, 2, n_c)


def solution(mesh):
    sizes = plane_sizes(mesh)
    if sizes is None:
        body, seq = general_shards, ("rep", "fs")
        weight = ("fs",)
        used = mesh
    else:
        body, seq = plane_shards(sizes), ("rep", "z", "y")
        weight = ("z", "y")
        used = Mesh(mesh.devices.reshape(sizes), ("rep", "z", "y", "tp"))
    placed = (
        P(seq, "tp"),
        P(),
        P(weight, "tp"),
        P(weight, "tp"),
        P(weight, "tp"),
        P(weight, "tp"),
        P(weight, "tp"),
        P("tp"),
        P(seq, "tp"),
        P("tp"),
        P("tp", weight),
        P(),
        P(weight, "tp"),
        P(weight, "tp"),
        P(None, "tp"),
        P(None, "tp"),
        P("tp", weight),
    )
    return jax.shard_map(body, mesh=used, in_specs=placed, out_specs=P(seq, "tp"), check_vma=False)
```

```python
import jax
import jax.numpy as jnp
from jax import lax
from jax.experimental import pallas as pl
from jax.experimental.pallas import tpu as pltpu
from jax.sharding import Mesh
from jax.sharding import PartitionSpec as P


HEAD_K = 32
HEAD_V = 64
BLOCK = 64
SUB = 8
LANES = 128

norm_eps = 1e-06
switch_multiplier = 16.0


def row_norm(content_tokens, gain):
    content_tokens = content_tokens.astype(jnp.float32)
    scaled = content_tokens * lax.rsqrt(
        jnp.mean(content_tokens * content_tokens, axis=-1, keepdims=True) + norm_eps
    )
    return (scaled * gain.astype(jnp.float32)).astype(jnp.bfloat16)


def gated_scan(probe_tokens, lookup_tokens, content_tokens, forgetting_scores):
    length, heads, key_size = probe_tokens.shape
    value_size = content_tokens.shape[-1]
    blocks = length // BLOCK

    def split_blocks(array):
        return array.reshape(blocks, BLOCK, heads, array.shape[-1])

    causal = jnp.arange(BLOCK)[:, None] >= jnp.arange(BLOCK)[None, :]
    highest = lax.Precision.HIGHEST

    def step(state, incoming_tokens):
        query_block, key_block, value_block, decay_block = incoming_tokens
        cumulative = jnp.cumsum(decay_block, axis=0)
        differ = cumulative[:, None] - cumulative[None, :]
        weight = jnp.exp(jnp.where(causal[:, :, None, None], differ, -jnp.inf))
        scores = jnp.einsum("thd,shd,tshd->tsh", query_block, key_block, weight, precision=highest)
        inner = jnp.einsum("tsh,shv->thv", scores, value_block, precision=highest)
        carried = jnp.einsum(
            "thd,hdv->thv", query_block * jnp.exp(cumulative), state, precision=highest
        )
        final = cumulative[-1]
        state = jnp.exp(final)[:, :, None] * state + jnp.einsum(
            "shd,shv->hdv",
            key_block * jnp.exp(final[None] - cumulative),
            value_block,
            precision=highest,
        )
        return (state, inner + carried)

    start_state = jnp.zeros((heads, key_size, value_size), jnp.float32)
    _, result_tokens = lax.scan(
        step,
        start_state,
        (
            split_blocks(probe_tokens),
            split_blocks(lookup_tokens),
            split_blocks(content_tokens),
            split_blocks(forgetting_scores),
        ),
    )
    return result_tokens.reshape(length, heads, value_size)


def attend_unit_results(
    probe_tokens,
    lookup_tokens,
    content_tokens,
    result_switch,
    forgetting_raw,
    spike_forgetting,
    attend_unit_scale,
):
    length = probe_tokens.shape[0]
    heads = probe_tokens.shape[1] // HEAD_K
    forgetting_scores = jax.nn.log_sigmoid(forgetting_raw) / switch_multiplier + spike_forgetting

    def split_heads(array, width):
        return array.astype(jnp.float32).reshape(length, heads, width)

    result_tokens = gated_scan(
        split_heads(probe_tokens, HEAD_K) * HEAD_K ** (-0.5),
        split_heads(lookup_tokens, HEAD_K),
        split_heads(content_tokens, HEAD_V),
        split_heads(forgetting_scores, HEAD_K),
    )
    result_tokens = result_tokens * lax.rsqrt(
        jnp.mean(result_tokens * result_tokens, axis=-1, keepdims=True) + norm_eps
    )
    result_tokens = result_tokens * attend_unit_scale.astype(jnp.float32).reshape(heads, HEAD_V)
    switched_result = result_tokens.reshape(length, heads * HEAD_V) * jax.nn.silu(
        result_switch.astype(jnp.float32)
    )
    return switched_result.astype(jnp.bfloat16)


def causal_conv(content_tokens, taps):
    content_tokens = content_tokens.astype(jnp.float32)
    taps = taps.astype(jnp.float32)
    width = taps.shape[0]
    padded = jnp.pad(content_tokens, ((width - 1, 0), (0, 0)))
    total = jnp.zeros_like(content_tokens)
    for offset in range(width):
        total = total + padded[offset : offset + content_tokens.shape[0]] * taps[offset]
    return total


def general_shards(
    incoming_features,
    attend_prenormal_scale,
    probe_matrix,
    lookup_matrix,
    content_matrix,
    forgetting_matrix,
    result_switch_matrix,
    forgetting_shift,
    spike_forget_logarithm,
    attend_unit_scale,
    attend_result_matrix,
    perceptron_scale,
    content_expand_matrix,
    switch_expand_matrix,
    content_kernel,
    switch_kernel,
    contract_matrix,
):
    whole_in = lax.all_gather(incoming_features, "tp", axis=1, tiled=True)
    columns = row_norm(whole_in, attend_prenormal_scale)
    pieces = tuple(
        lax.all_gather(piece, "fs", axis=0, tiled=True)
        for piece in (
            probe_matrix,
            lookup_matrix,
            content_matrix,
            forgetting_matrix,
            result_switch_matrix,
        )
    )
    query_sum, key_sum, value_sum, decay_sum, gate_sum = tuple(
        (jnp.dot(columns, piece, preferred_element_type=jnp.float32) for piece in pieces)
    )
    switched_result = attend_unit_results(
        query_sum.astype(jnp.bfloat16),
        key_sum.astype(jnp.bfloat16),
        value_sum.astype(jnp.bfloat16),
        gate_sum.astype(jnp.bfloat16),
        decay_sum + forgetting_shift,
        spike_forget_logarithm,
        attend_unit_scale,
    )
    mixer_partial = jnp.dot(
        switched_result,
        lax.all_gather(attend_result_matrix, "fs", axis=1, tiled=True),
        preferred_element_type=jnp.float32,
    )
    mix = lax.psum_scatter(
        mixer_partial.astype(jnp.bfloat16), "tp", scatter_dimension=1, tiled=True
    )
    middle = (
        incoming_features.astype(jnp.float32) + lax.optimization_barrier(mix).astype(jnp.float32)
    ).astype(jnp.bfloat16)
    whole_mid = lax.all_gather(middle, "tp", axis=1, tiled=True)
    columns = row_norm(whole_mid, perceptron_scale)
    pieces = (
        lax.all_gather(content_expand_matrix, "fs", axis=0, tiled=True),
        lax.all_gather(switch_expand_matrix, "fs", axis=0, tiled=True),
    )
    value_total = jnp.dot(columns, pieces[0], preferred_element_type=jnp.float32)
    gate_total = jnp.dot(columns, pieces[1], preferred_element_type=jnp.float32)
    conv_value = causal_conv(value_total.astype(jnp.bfloat16), content_kernel)
    conv_gated = causal_conv(gate_total.astype(jnp.bfloat16), switch_kernel)
    hidden = (conv_value * jax.nn.gelu(conv_gated, approximate=True)).astype(jnp.bfloat16)
    down_partial = jnp.dot(
        hidden,
        lax.all_gather(contract_matrix, "fs", axis=1, tiled=True),
        preferred_element_type=jnp.float32,
    )
    ffn = lax.psum_scatter(down_partial.astype(jnp.bfloat16), "tp", scatter_dimension=1, tiled=True)
    return (middle.astype(jnp.float32) + lax.optimization_barrier(ffn).astype(jnp.float32)).astype(
        jnp.bfloat16
    )


F32 = jnp.float32
BF16 = jnp.bfloat16


def dot(a, b):
    return jnp.dot(a, b, preferred_element_type=F32)


def pack_kernel(pos, probe, lookup, content, forget, switch, result, own, send):
    quarter, across = pos[0], pos[1]
    rows = probe.shape[0]
    half = rows // 2
    key_w = probe.shape[1] // 4
    val_w = content.shape[1] // 4
    part = result.shape[0] // 4

    def pack(index, out):
        for q in range(4):

            @pl.when(index == q)
            def _():
                keys = pl.ds(q * key_w, key_w)
                vals = pl.ds(q * val_w, val_w)
                out[0:rows, :] = jnp.concatenate([probe[:, keys], lookup[:, keys]], axis=1)
                out[rows : 2 * rows, :] = content[:, vals]
                out[2 * rows : 3 * rows, :] = switch[:, vals]
                base = 3 * rows
                out[base : base + part, :] = result[q * part : (q + 1) * part, 0:LANES]
                out[base + part : base + 2 * part, :] = result[q * part : (q + 1) * part, LANES:]
                base = base + 2 * part
                decay = forget[:, keys]
                out[base : base + half, :] = jnp.concatenate(
                    [decay[:half], decay[half:]], axis=1
                )

    pack(across, send)
    pack(quarter, own)


def input_kernel(pos, spike, feat, own_spike, to_x, to_y, to_d):
    key_w = spike.shape[1] // 4
    width = feat.shape[1]

    def spikes(index):
        value = spike[:, 0:key_w]
        for q in range(1, 4):
            value = jnp.where(index == q, spike[:, q * key_w : (q + 1) * key_w], value)
        high = value.astype(BF16)
        low = (value - high.astype(F32)).astype(BF16)
        return jnp.concatenate([high, low], axis=1)

    own_spike[...] = spikes(pos[0])
    for slot, ref in ((2, to_x), (3, to_y), (4, to_d)):
        ref[:, 0:width] = feat[...]
        ref[:, width:] = spikes(pos[slot])


def copy_from(choices, sem, dst, cut):
    for cond, ref in choices:
        copy = pltpu.make_async_copy(cut(ref), dst, sem)
        if cond is None:
            copy.start()
        else:
            pl.when(cond)(copy.start)


def blocks_of(pos, slots):
    slot_o, slot_r1, slot_l1, slot_r2, slot_l2, slot_r3, slot_l3 = slots
    z, last = pos[6], pos[8]
    low = z < 2
    first_z = z == 0
    last_z = z == last
    return (
        (z, ((None, slot_o),)),
        (jnp.bitwise_xor(z, 2), ((low, slot_l2), (jnp.logical_not(low), slot_r2))),
        (
            jnp.where(first_z, last, z - 1),
            ((first_z, slot_l3), (jnp.logical_not(first_z), slot_r1)),
        ),
        (
            jnp.where(last_z, 0, z + 1),
            ((last_z, slot_r3), (jnp.logical_not(last_z), slot_l1)),
        ),
    )


def attend_kernel(
    pos, mine, theirs, scale, shift, unit, spike_o, spike_x, spike_y, spike_d,
    slot_o, slot_r1, slot_l1, slot_r2, slot_l2, slot_r3, slot_l3,
    keep, send,
    w_qk, w_vg, w_f, w_o, folded, qk_s, v_s, g_s, f_s, gated, sems,
):
    core, y = pos[5], pos[7]
    rows = slot_o.shape[0] // 2
    chunk = w_qk.shape[0] // 8
    half = chunk // 2
    part = w_o.shape[1]
    span = spike_o.shape[0]
    length, width = mine.shape
    key_w = f_s.shape[1] // 2

    slots = (slot_o, slot_r1, slot_l1, slot_r2, slot_l2, slot_r3, slot_l3)
    waits = []
    for index, (zi, choices) in enumerate(blocks_of(pos, slots)):
        for j in range(2):
            shard = zi * 2 + (y if j == 0 else 1 - y)
            at = pl.ds(pl.multiple_of(shard * chunk, chunk), chunk)
            base = j * rows
            targets = (
                (w_qk.at[at, :], chunk),
                (w_vg.at[at, 0:LANES], chunk),
                (w_vg.at[at, LANES : 2 * LANES], chunk),
                (w_o.at[shard, :, 0:LANES], part),
                (w_o.at[shard, :, LANES : 2 * LANES], part),
                (folded.at[shard], half),
            )
            for k, (dst, size) in enumerate(targets):
                sem = sems.at[index * 12 + j * 6 + k]
                copy_from(choices, sem, dst, lambda ref, b=base, n=size: ref.at[pl.ds(b, n), :])
                waits.append((slot_o.at[pl.ds(base, size), :], dst, sem))
                base += size
    for source, dst, sem in waits:
        pltpu.make_async_copy(source, dst, sem).wait()
    for shard in range(8):
        w_f[shard * chunk : shard * chunk + half, :] = folded[shard]
        w_f[shard * chunk + half : (shard + 1) * chunk, :] = pltpu.roll(
            folded[shard].astype(F32), key_w, 1
        ).astype(BF16)

    def project(s, carry):
        at = pl.ds(pl.multiple_of(s * span, span), span)
        a = mine[at, :].astype(F32)
        b = theirs[at, :].astype(F32)
        total = jnp.sum(a * a, axis=1, keepdims=True) + jnp.sum(b * b, axis=1, keepdims=True)
        inverse = lax.rsqrt(total / scale.shape[1] + norm_eps)
        low = jnp.where(core == 0, a, b)
        high = jnp.where(core == 0, b, a)
        width = a.shape[1]
        normed = jnp.concatenate(
            [
                (low * inverse * scale[:, 0:width].astype(F32)).astype(BF16),
                (high * inverse * scale[:, width:].astype(F32)).astype(BF16),
            ],
            axis=1,
        )
        qk_s[at, :] = dot(normed, w_qk[...]).astype(BF16).astype(F32)
        vg = dot(normed, w_vg[...]).astype(BF16)
        v_s[at, :] = vg[:, 0:LANES]
        g_s[at, :] = vg[:, LANES:]
        f_s[at, :] = dot(normed, w_f[...])
        return carry

    count = length // span
    lax.fori_loop(0, count, project, 0)

    lane = lax.broadcasted_iota(jnp.int32, (span, LANES), 1)
    left = lane < key_w
    row = lax.broadcasted_iota(jnp.int32, (span, LANES), 0)
    lane_head = lax.broadcasted_iota(jnp.int32, (LANES, 2 * LANES), 0) // HEAD_K
    wide_head = lax.broadcasted_iota(jnp.int32, (LANES, 2 * LANES), 1) // HEAD_V
    spread = (lane_head == wide_head).astype(BF16)
    wide_a = lax.broadcasted_iota(jnp.int32, (2 * LANES, 2 * LANES), 0) // HEAD_V
    wide_b = lax.broadcasted_iota(jnp.int32, (2 * LANES, 2 * LANES), 1) // HEAD_V
    same_wide = (wide_a == wide_b).astype(BF16)
    tri = (
        lax.broadcasted_iota(jnp.int32, (span, span), 0)
        >= lax.broadcasted_iota(jnp.int32, (span, span), 1)
    ).astype(BF16)
    heads = LANES // HEAD_K
    key_heads = lax.broadcasted_iota(jnp.int32, (1, LANES), 1) // HEAD_K
    value_heads = lax.broadcasted_iota(jnp.int32, (1, 2 * LANES), 1) // HEAD_V

    def split_dot(a, value):
        one = value.astype(BF16)
        rest = value - one.astype(F32)
        two = rest.astype(BF16)
        three = (rest - two.astype(F32)).astype(BF16)
        return dot(a, one) + dot(a, two) + dot(a, three)

    def pair(p, carry):
        at_a = pl.ds(pl.multiple_of(p * 2 * span, span), span)
        at_b = pl.ds(pl.multiple_of(p * 2 * span + span, span), span)
        qk_a, qk_b = qk_s[at_a, :], qk_s[at_b, :]
        query = jnp.where(left, qk_a, pltpu.roll(qk_b, key_w, 1)) * HEAD_K ** (-0.5)
        keys = jnp.where(left, pltpu.roll(qk_a, key_w, 1), qk_b)
        v_a, v_b = v_s[at_a, :], v_s[at_b, :]
        value = jnp.concatenate([v_a, v_b], axis=1)
        decay = jnp.where(left, f_s[at_a, :], pltpu.roll(f_s[at_b, :], key_w, 1))
        decay = decay + shift[...]
        spike_a = jnp.where(p == 0, spike_o[...], spike_y[:, width:]).astype(F32)
        spike_b = jnp.where(p == 0, spike_x[:, width:], spike_d[:, width:]).astype(F32)
        spike_a = spike_a + pltpu.roll(spike_a, key_w, 1)
        spike_b = spike_b + pltpu.roll(spike_b, key_w, 1)
        soft = jnp.minimum(decay, 0.0) - jnp.log1p(jnp.exp(-jnp.abs(decay)))
        log_decay = soft / switch_multiplier + jnp.where(left, spike_a, spike_b)
        cum = split_dot(tri, log_decay)

        tiles = span // SUB
        q3 = query.reshape(tiles, SUB, LANES)
        k3 = keys.reshape(tiles, SUB, LANES)
        c3 = cum.reshape(tiles, SUB, LANES)
        valuef = value.astype(F32)
        v3 = valuef.reshape(tiles, SUB, 2 * LANES)
        place = lax.broadcasted_iota(jnp.int32, (tiles, SUB, LANES), 1)
        out = jnp.zeros((span, 2 * LANES), F32)
        for lag in range(SUB):
            if lag == 0:
                term = q3 * k3
                v_lag = v3
            else:
                k_lag = pltpu.roll(k3, lag, 1)
                c_lag = pltpu.roll(c3, lag, 1)
                v_lag = pltpu.roll(v3, lag, 1)
                fall = jnp.exp(jnp.where(place >= lag, c3 - c_lag, -jnp.inf))
                term = q3 * k_lag * fall
            spread_term = dot(term.reshape(span, LANES).astype(BF16), spread)
            out = out + spread_term * v_lag.reshape(span, 2 * LANES)

        size = SUB
        while size < span:
            blocks = max(span // (2 * size), 1)
            if 2 * size > span:
                second_rows = span - size
            else:
                second_rows = size
            begin = [i * 2 * size for i in range(blocks)]
            q_parts, k_parts, v_parts = [], [], []
            for b0 in begin:
                middle = b0 + size
                ref_row = cum[middle - 1 : middle, :]
                q_parts.append(
                    query[middle : middle + second_rows]
                    * jnp.exp(cum[middle : middle + second_rows] - ref_row)
                )
                k_parts.append(keys[b0:middle] * jnp.exp(ref_row - cum[b0:middle]))
                v_parts.append(value[b0:middle] if size % 16 == 0 else valuef[b0:middle])
            q_all = jnp.concatenate(q_parts, axis=0) if blocks > 1 else q_parts[0]
            k_all = jnp.concatenate(k_parts, axis=0) if blocks > 1 else k_parts[0]
            v_all = (jnp.concatenate(v_parts, axis=0) if blocks > 1 else v_parts[0]).astype(BF16)
            n_q, n_k = q_all.shape[0], k_all.shape[0]
            q_heads = jnp.concatenate(
                [jnp.where(key_heads == h, q_all, 0.0).astype(BF16) for h in range(heads)],
                axis=0,
            )
            scores = lax.dot_general(
                q_heads, k_all.astype(BF16), (((1,), (1,)), ((), ())), preferred_element_type=F32
            )
            if blocks > 1:
                shift_by = size.bit_length() - 1
                q_block = lax.shift_right_logical(
                    lax.broadcasted_iota(jnp.int32, (n_q, n_k), 0), shift_by
                )
                k_block = lax.shift_right_logical(
                    lax.broadcasted_iota(jnp.int32, (n_q, n_k), 1), shift_by
                )
                same_block = (q_block == k_block).astype(F32)
                scores = scores * jnp.concatenate([same_block] * heads, axis=0)
            wide = dot(scores.astype(BF16), v_all)
            total = wide[0:n_q]
            for h in range(1, heads):
                total = jnp.where(value_heads == h, wide[h * n_q : (h + 1) * n_q], total)
            zeros = jnp.zeros((size, 2 * LANES), F32)
            full = []
            for i in range(blocks):
                full.append(zeros)
                full.append(total[i * second_rows : (i + 1) * second_rows])
            covered = blocks * size + blocks * second_rows
            if covered < span:
                full.append(jnp.zeros((span - covered, 2 * LANES), F32))
            out = out + jnp.concatenate(full, axis=0)
            size *= 2

        square = out * out
        high = square.astype(BF16)
        low = (square - high.astype(F32)).astype(BF16)
        mean = (dot(high, same_wide) + dot(low, same_wide)) / HEAD_V
        out = out * lax.rsqrt(mean + norm_eps)
        gate = jnp.concatenate([g_s[at_a, :], g_s[at_b, :]], axis=1).astype(F32)
        gain = unit[...].astype(F32)
        out = out * jnp.concatenate([gain, gain], axis=1)
        out = out * (gate / (1.0 + jnp.exp(-gate)))
        gated[at_a, :] = out[:, 0:LANES].astype(BF16)
        gated[at_b, :] = out[:, LANES:].astype(BF16)
        return carry

    lax.fori_loop(0, count // 2, pair, 0)
    mix_out(core, gated, w_o, keep, send)


def mix_out(core, left, weights, keep, send):
    shards = weights.shape[0]
    width = weights.shape[2]
    for h in range(2):
        for f in range(shards // 2):
            w = weights[h * (shards // 2) + f]
            value = dot(left[...], w).astype(BF16)
            cols = slice(f * width, (f + 1) * width)

            @pl.when(core == h)
            def _():
                keep[:, cols] = value

            @pl.when(core != h)
            def _():
                send[:, cols] = value


def expand_kernel(
    pos, mine, theirs, scale, taps_v, taps_g,
    *refs,
):
    own, received = refs[0:7], refs[7:14]
    hidden, w_up, sems = refs[14:]
    core, y = pos[5], pos[7]
    chunk = own[0].shape[0]
    span = hidden.shape[0] // 4
    width = hidden.shape[1]

    waits = []
    for j, slots in enumerate((own, received)):
        side = y if j == 0 else 1 - y
        for index, (zi, choices) in enumerate(blocks_of(pos, slots)):
            dst = w_up.at[pl.ds(pl.multiple_of((zi * 2 + side) * chunk, chunk), chunk), :]
            sem = sems.at[index * 2 + j]
            copy_from(choices, sem, dst, lambda ref: ref)
            waits.append((slots[0], dst, sem))
    for source, dst, sem in waits:
        pltpu.make_async_copy(source, dst, sem).wait()

    def conv(value, taps):
        taps = taps.astype(F32)
        row = lax.broadcasted_iota(jnp.int32, value.shape, 0)
        total = value * taps[2:3]
        total = total + jnp.where(row >= 1, pltpu.roll(value, 1, 0), 0.0) * taps[1:2]
        return total + jnp.where(row >= 2, pltpu.roll(value, 2, 0), 0.0) * taps[0:1]

    def sequence(s, carry):
        at = pl.ds(pl.multiple_of(s * span, span), span)
        a = mine[at, :].astype(F32)
        b = theirs[at, :].astype(F32)
        total = jnp.sum(a * a, axis=1, keepdims=True) + jnp.sum(b * b, axis=1, keepdims=True)
        inverse = lax.rsqrt(total / scale.shape[1] + norm_eps)
        low = jnp.where(core == 0, a, b)
        high = jnp.where(core == 0, b, a)
        half = a.shape[1]
        normed = jnp.concatenate(
            [
                (low * inverse * scale[:, 0:half].astype(F32)).astype(BF16),
                (high * inverse * scale[:, half:].astype(F32)).astype(BF16),
            ],
            axis=1,
        )
        value = dot(normed, w_up[:, 0:width]).astype(BF16).astype(F32)
        gate = dot(normed, w_up[:, width:]).astype(BF16).astype(F32)
        value = conv(value, taps_v[...])
        gate = conv(gate, taps_g[...])
        hidden[at, :] = (value * jax.nn.gelu(gate, approximate=True)).astype(BF16)
        return carry

    lax.fori_loop(0, 4, sequence, 0)


def contract_kernel(
    pos, hidden, slot_o, slot_r1, slot_l1, slot_r2, slot_l2, slot_r3, slot_l3,
    keep, send, weights, sems,
):
    core = pos[5]
    width = weights.shape[3]
    slots = (slot_o, slot_r1, slot_l1, slot_r2, slot_l2, slot_r3, slot_l3)
    waits = []
    for index, (zi, choices) in enumerate(blocks_of(pos, slots)):
        dst = weights.at[jnp.where((zi // 2) == core, 0, 1), lax.rem(zi, 2)]
        sem = sems.at[index]
        copy_from(choices, sem, dst, lambda ref: ref)
        waits.append((slot_o, dst, sem))
    for source, dst, sem in waits:
        pltpu.make_async_copy(source, dst, sem).wait()
    for index, out in ((1, send), (0, keep)):
        for low in range(2):
            out[:, low * width : (low + 1) * width] = dot(
                hidden[...], weights[index, low]
            ).astype(BF16)


def call(kernel, outs, args, scratch=(), flops=0, free=0, grant=24, fixed=False):
    in_specs = [pl.BlockSpec(memory_space=pltpu.SMEM)]
    in_specs += [pl.BlockSpec(memory_space=pltpu.VMEM)] * (len(args) - 1 - free)
    in_specs += [pl.BlockSpec(memory_space=pltpu.HBM if fixed else pl.ANY)] * free
    return pl.pallas_call(
        kernel,
        out_shape=[jax.ShapeDtypeStruct(*o) for o in outs],
        in_specs=in_specs,
        out_specs=[pl.BlockSpec(memory_space=pltpu.VMEM)] * len(outs),
        scratch_shapes=list(scratch),
        cost_estimate=pl.CostEstimate(flops=flops, bytes_accessed=1 << 20, transcendentals=0),
        compiler_params=pltpu.CompilerParams(vmem_limit_bytes=grant << 20),
    )(*args)


def plane_shards(sizes):
    n_x, n_z, n_y, n_c = sizes
    axes = ("rep", "z", "y", "tp")

    def pairs(move):
        found = []
        for x in range(n_x):
            for z in range(n_z):
                for y in range(n_y):
                    for c in range(n_c):
                        to = move(x, z, y, c)
                        if to is not None:
                            a = ((x * n_z + z) * n_y + y) * n_c + c
                            b = ((to[0] * n_z + to[1]) * n_y + to[2]) * n_c + to[3]
                            found.append((a, b))
        return found

    over_x = pairs(lambda x, z, y, c: (1 - x, z, y, c))
    over_y = pairs(lambda x, z, y, c: (x, z, 1 - y, c))
    over_d = pairs(lambda x, z, y, c: (1 - x, z, 1 - y, c))
    over_c = pairs(lambda x, z, y, c: (x, z, y, 1 - c))
    up_z = pairs(lambda x, z, y, c: (x, z + 1, y, c) if z + 1 < n_z else None)
    down_z = pairs(lambda x, z, y, c: (x, z - 1, y, c) if z > 0 else None)
    up_z2 = pairs(lambda x, z, y, c: (x, z + 1, y, c) if 1 <= z < n_z - 1 else None)
    down_z2 = pairs(lambda x, z, y, c: (x, z - 1, y, c) if 0 < z < n_z - 1 else None)
    up_z3 = pairs(lambda x, z, y, c: (x, z + 1, y, c) if z == n_z - 2 else None)
    down_z3 = pairs(lambda x, z, y, c: (x, z - 1, y, c) if z == 1 else None)

    up_z3_direct = pairs(lambda x, z, y, c: (x, n_z - 1, y, c) if z == n_z - 3 else None)
    down_z3_direct = pairs(lambda x, z, y, c: (x, 0, y, c) if z == 2 else None)

    def move(value, perm):
        return lax.ppermute(value, axes, perm)

    def gather(slot, direct=False):
        r1 = move(slot, up_z)
        l1 = move(slot, down_z)
        r2 = move(r1, up_z2)
        l2 = move(l1, down_z2)
        if direct:
            r3 = move(r1, up_z3_direct)
            l3 = move(l1, down_z3_direct)
        else:
            r3 = move(r2, up_z3)
            l3 = move(l2, down_z3)
        return slot, r1, l1, r2, l2, r3, l3

    def shards(
        incoming_features,
        attend_prenormal_scale,
        probe_matrix,
        lookup_matrix,
        content_matrix,
        forgetting_matrix,
        result_switch_matrix,
        forgetting_shift,
        spike_forget_logarithm,
        attend_unit_scale,
        attend_result_matrix,
        perceptron_scale,
        content_expand_matrix,
        switch_expand_matrix,
        content_kernel,
        switch_kernel,
        contract_matrix,
    ):
        x, z, y, c = (lax.axis_index(axis) for axis in axes)
        quarter = 2 * x + y
        pos = jnp.stack(
            [
                quarter,
                2 * x + (1 - y),
                2 * (1 - x) + y,
                2 * x + (1 - y),
                2 * (1 - x) + (1 - y),
                c,
                z,
                y,
                jnp.int32(n_z - 1),
            ]
        ).astype(jnp.int32)
        span, width = incoming_features.shape
        embed = width * n_c
        chunk = probe_matrix.shape[0]
        part = attend_result_matrix.shape[0] // 4
        pack_rows = 3 * chunk + 2 * part + chunk // 2
        own, send = call(
            pack_kernel,
            [((pack_rows, LANES), BF16)] * 2,
            (
                pos,
                probe_matrix,
                lookup_matrix,
                content_matrix,
                forgetting_matrix,
                result_switch_matrix,
                attend_result_matrix,
            ),
            grant=56,
        )
        spike_o, to_x, to_y, to_d = call(
            input_kernel,
            [((span, LANES), BF16)] + [((span, width + LANES), BF16)] * 3,
            (pos, spike_forget_logarithm, incoming_features),
            grant=56,
        )
        attn = gather(jnp.concatenate([own, move(send, over_y)], axis=0))
        from_x = move(to_x, over_x)
        from_y = move(to_y, over_y)
        from_d = move(to_d, over_d)

        ff = content_expand_matrix.shape[1] // 4

        def up_part(index):
            return jnp.concatenate(
                [
                    lax.dynamic_slice_in_dim(content_expand_matrix, index * ff, ff, 1),
                    lax.dynamic_slice_in_dim(switch_expand_matrix, index * ff, ff, 1),
                ],
                axis=1,
            )

        def down_part(index):
            return lax.dynamic_slice_in_dim(contract_matrix, index * ff, ff, 0)

        across = 2 * x + (1 - y)
        up = gather(up_part(quarter))
        up = up + gather(move(up_part(across), over_y))
        kept, received = down_part(quarter), move(down_part(across), over_y)
        down_own = gather(jnp.where(y == 0, kept, received), direct=True)
        down_across = gather(jnp.where(y == 0, received, kept), direct=True)

        def halves(blocks):
            mine = jnp.concatenate(blocks, axis=0)
            return mine, move(mine, over_c)

        def reduce(keep, other):
            total = (keep.astype(F32) + other.astype(F32)).astype(BF16)
            blocks = [total[i * span : (i + 1) * span] for i in range(4)]
            return (
                blocks[0], move(blocks[1], over_x), move(blocks[2], over_y), move(blocks[3], over_d)
            )

        def add_up(base, parts):
            total = parts[0].astype(F32)
            for part_ in parts[1:]:
                total = total + part_.astype(F32)
            return (base.astype(F32) + total.astype(BF16).astype(F32)).astype(BF16)

        tokens = 4 * span
        mine, theirs = halves(
            [incoming_features] + [value[:, :width] for value in (from_x, from_y, from_d)],
        )
        key_w = forgetting_shift.shape[0] // 4
        val_w = attend_unit_scale.shape[0] // 4
        shift = lax.dynamic_slice_in_dim(forgetting_shift, quarter * key_w, key_w, 0)
        shift = jnp.concatenate([shift, shift]).reshape(1, LANES)
        unit = lax.dynamic_slice_in_dim(attend_unit_scale, quarter * val_w, val_w, 0)
        unit = unit.reshape(1, val_w)
        before = attend_prenormal_scale.reshape(1, embed)
        after = perceptron_scale.reshape(1, embed)
        keep, other = call(
            attend_kernel,
            [((tokens, width), BF16)] * 2,
            (
                pos,
                mine,
                theirs,
                before,
                shift,
                unit,
                spike_o,
                from_x,
                from_y,
                from_d,
            )
            + attn,
            scratch=[
                pltpu.VMEM((embed, LANES), BF16),
                pltpu.VMEM((embed, 2 * LANES), BF16),
                pltpu.VMEM((embed, LANES), BF16),
                pltpu.VMEM((8, part, embed // 8), BF16),
                pltpu.VMEM((8, chunk // 2, LANES), BF16),
                pltpu.VMEM((tokens, LANES), F32),
                pltpu.VMEM((tokens, LANES), BF16),
                pltpu.VMEM((tokens, LANES), BF16),
                pltpu.VMEM((tokens, LANES), F32),
                pltpu.VMEM((tokens, LANES), BF16),
                pltpu.SemaphoreType.DMA((48,)),
            ],
            fixed=True,
            flops=10**10,
            free=7,
        )
        middle = add_up(incoming_features, reduce(keep, move(other, over_c)))
        mine, theirs = halves(
            [middle, move(middle, over_x), move(middle, over_y), move(middle, over_d)],
        )
        taps_v = lax.dynamic_slice_in_dim(content_kernel, quarter * ff, ff, 1)
        taps_g = lax.dynamic_slice_in_dim(switch_kernel, quarter * ff, ff, 1)
        (hidden,) = call(
            expand_kernel,
            [((tokens, ff), BF16)],
            (pos, mine, theirs, after, taps_v, taps_g) + up,
            scratch=[pltpu.VMEM((embed, 2 * ff), BF16), pltpu.SemaphoreType.DMA((8,))],
            flops=10**10,
            free=14,
        )
        half = width // 2
        parts = []
        for slots in (down_own, down_across):
            keep, other = call(
                contract_kernel,
                [((tokens, half), BF16)] * 2,
                (pos, hidden) + slots,
                scratch=[
                    pltpu.VMEM((2, 2, ff, embed // 8), BF16),
                    pltpu.SemaphoreType.DMA((4,)),
                ],
                flops=10**10,
                free=7,
            )
            pieces = reduce(keep, move(other, over_c))
            total = pieces[0].astype(F32)
            for piece in pieces[1:]:
                total = total + piece.astype(F32)
            parts.append(total.astype(BF16).astype(F32))
        shard = half // 2
        first, second = parts
        ffn = jnp.concatenate(
            [first[:, :shard], second[:, :shard], first[:, shard:], second[:, shard:]], axis=1
        )
        return (middle.astype(F32) + ffn).astype(BF16)

    return shards


def plane_sizes(mesh):
    if tuple(mesh.axis_names) != ("rep", "fs", "tp"):
        return None
    n_x, n_fs, n_c = (mesh.shape[axis] for axis in ("rep", "fs", "tp"))
    if n_x != 2 or n_c != 2 or n_fs % 2 or n_fs // 2 != 4:
        return None
    return (n_x, n_fs // 2, 2, n_c)


def solution(mesh):
    sizes = plane_sizes(mesh)
    if sizes is None:
        body, seq = general_shards, ("rep", "fs")
        weight = ("fs",)
        used = mesh
    else:
        body, seq = plane_shards(sizes), ("rep", "z", "y")
        weight = ("z", "y")
        used = Mesh(mesh.devices.reshape(sizes), ("rep", "z", "y", "tp"))
    placed = (
        P(seq, "tp"),
        P(),
        P(weight, "tp"),
        P(weight, "tp"),
        P(weight, "tp"),
        P(weight, "tp"),
        P(weight, "tp"),
        P("tp"),
        P(seq, "tp"),
        P("tp"),
        P("tp", weight),
        P(),
        P(weight, "tp"),
        P(weight, "tp"),
        P(None, "tp"),
        P(None, "tp"),
        P("tp", weight),
    )
    return jax.shard_map(body, mesh=used, in_specs=placed, out_specs=P(seq, "tp"), check_vma=False)
```
